32 devices in a mesh: sp: 8 (over z, y), tp: 4 (over x, core).
Axes of the slice: x: 2, y: 2, z: 4, core: 2. Of those that a mesh axis runs over, the one named last changes fastest.
Arguments:
- resid_in: bfloat16 [2048, 2048], P('sp'), may hold values from -6 to 6
- query_latent: bfloat16 [2048, 768], P('sp'), may hold values from -6 to 6
- kv_latent: bfloat16 [2048, 512], P('sp'), may hold values from -6 to 6
- rotary_key: bfloat16 [2048, 64], P('sp'), may hold values from -200 to 200
- query_gain: float32 [768], replicated, may hold values from 0.1 to 1.9
- kv_gain: float32 [512], replicated, may hold values from 0.1 to 1.9
- w_query_plain: bfloat16 [768, 2048], P(None, 'tp'), may hold values from -0.875 to 0.875
- w_query_rotary: bfloat16 [768, 1024], P(None, 'tp'), may hold values from -0.875 to 0.875
- w_key_plain: bfloat16 [512, 2048], P(None, 'tp'), may hold values from -0.25 to 0.25
- w_value: bfloat16 [512, 2048], P(None, 'tp'), may hold values from -0.25 to 0.25
- w_output: bfloat16 [2048, 2048], P('tp'), may hold values from -0.125 to 0.125
- ffn_gain: float32 [2048], replicated, may hold values from 0.1 to 1.9
- w_gate: bfloat16 [2048, 5632], P('sp', 'tp'), may hold values from -0.125 to 0.125
- w_up: bfloat16 [2048, 5632], P('sp', 'tp'), may hold values from -0.125 to 0.125
- w_down: bfloat16 [5632, 2048], P('tp', 'sp'), may hold values from -0.078125 to 0.078125
Outputs:
- resid_out: bfloat16 [2048, 2048], P(('sp', 'tp'))
The draws below stay inside these ranges and needn't reach their ends.
All inputs are finite; a program needn't handle non-finite values.
Results may differ from the reference program's by a relative error of at most 0.014.
The reference program's roundings to bfloat16 on the way count: a program that leaves them out, or rounds other values in their place, can miss the bound.
Values may be sent and summed in bfloat16 or wider, within the bound.
A program may use at most 192 MiB of HBM per device.

```python
import jax
import jax.numpy as jnp
from jax import lax

D = 2048
HEADS = 16
QR = 768
KVR = 512
NOPE = 128
ROPE = 64
VDIM = 128
FF = 5632
TOK_DEV = 256
SEQ = 2048


def draw_rotary_key(key, part):
    first = jax.random.fold_in(jax.random.fold_in(key, 11), 0)
    base = jnp.clip(jax.random.normal(first, (SEQ, ROPE), jnp.float32), -5.0, 5.0)
    return base.astype(jnp.bfloat16)


def shard_levels(own_key, shape, cuts, smallest, top_value):
    factor_of = 1.0
    for dim, blocks in cuts:
        draws = jax.random.uniform(jax.random.fold_in(jax.random.fold_in(own_key, 6), dim), (blocks,), jnp.float32, smallest / len(cuts), top_value / len(cuts))
        factor_of = factor_of * jnp.repeat(jnp.exp(draws), shape[dim] // blocks).reshape((-1,) + (1,) * (len(shape) - 1 - dim))
    return factor_of


def normal_values(stream_key, dims, spread, most, cuts=(), kind=jnp.bfloat16):
    drawn = jax.random.normal(stream_key, dims, jnp.float32) * spread
    if len(cuts) > 0:
        drawn = shard_levels(stream_key, dims, cuts, -0.22, 0.18) * drawn
    return jnp.clip(drawn, min=-most, max=most).astype(kind)


def setup_inputs(seed: int = 0) -> dict:
    key_of = jax.random.split(jax.random.key(seed), 16)
    resid_in = normal_values(key_of[0], (SEQ, D), 1.0, 6.0, ((0, 8),))
    query_latent = normal_values(key_of[1], (SEQ, QR), 1.0, 6.0, ((0, 8),))
    kv_latent = normal_values(key_of[2], (SEQ, KVR), 1.0, 6.0, ((0, 8),))
    rotary_key = draw_rotary_key(jax.random.fold_in(key_of[15], 71), 0)
    query_gain = jnp.clip(1.0 + 0.18 * jax.random.normal(key_of[4], (QR,), jnp.float32), 0.1, 1.9)
    kv_gain = jnp.clip(1.0 + 0.18 * jax.random.normal(key_of[5], (KVR,), jnp.float32), 0.1, 1.9)
    w_query_plain = normal_values(key_of[6], (QR, HEADS * NOPE), (QR // 16) ** -0.5, 0.875, ((1, 4),))
    w_query_rotary = normal_values(key_of[7], (QR, HEADS * ROPE), (QR // 16) ** -0.5, 0.875, ((1, 4),))
    w_key_plain = normal_values(key_of[8], (KVR, HEADS * NOPE), KVR ** -0.5, 0.25, ((1, 4),))
    w_value = normal_values(key_of[9], (KVR, HEADS * VDIM), KVR ** -0.5, 0.25, ((1, 4),))
    w_output = normal_values(key_of[10], (HEADS * VDIM, D), (HEADS * VDIM) ** -0.5, 0.125, ((0, 4),))
    ffn_gain = jnp.clip(1.0 + 0.18 * jax.random.normal(key_of[11], (D,), jnp.float32), 0.1, 1.9)
    w_gate = normal_values(key_of[12], (D, FF), D ** -0.5, 0.125, ((0, 8), (1, 4)))
    w_up = normal_values(key_of[13], (D, FF), D ** -0.5, 0.125, ((0, 8), (1, 4)))
    w_down = normal_values(key_of[14], (FF, D), FF ** -0.5, 0.078125, ((0, 4), (1, 8)))
    return dict(resid_in=resid_in, query_latent=query_latent, kv_latent=kv_latent, rotary_key=rotary_key, query_gain=query_gain, kv_gain=kv_gain, w_query_plain=w_query_plain, w_query_rotary=w_query_rotary, w_key_plain=w_key_plain, w_value=w_value, w_output=w_output, ffn_gain=ffn_gain, w_gate=w_gate, w_up=w_up, w_down=w_down)


def normed(values, gain):
    wide = values.astype(jnp.float32)
    return wide * lax.rsqrt(lax.optimization_barrier(jnp.mean(wide * wide, axis=-1, keepdims=True)) + 1e-06) * gain.astype(jnp.float32)

def rotate(values, cosine, sine):
    half = values.shape[-1] // 2
    first = values[..., :half]
    second = values[..., half:]
    return jnp.concatenate([first * cosine - second * sine, second * cosine + first * sine], axis=-1)

def reference(resid_in, query_latent, kv_latent, rotary_key, query_gain, kv_gain, w_query_plain, w_query_rotary, w_key_plain, w_value, w_output, ffn_gain, w_gate, w_up, w_down):
    length = resid_in.shape[0]
    position = jnp.arange(length, dtype=jnp.float32)
    freq = 10000.0 ** (-jnp.arange(0, ROPE, 2, dtype=jnp.float32) / ROPE)
    angle = position[:, None] * freq[None, :]
    cosine = jnp.cos(angle)
    sine = jnp.sin(angle)
    q_norm = normed(query_latent, query_gain).astype(jnp.bfloat16)
    kv_norm = normed(kv_latent, kv_gain).astype(jnp.bfloat16)
    key_rot = rotate(rotary_key.astype(jnp.float32), cosine, sine).astype(jnp.bfloat16)
    q_plain = jnp.dot(q_norm, w_query_plain, preferred_element_type=jnp.float32).astype(jnp.bfloat16).reshape(length, HEADS, NOPE)
    q_raw = jnp.dot(q_norm, w_query_rotary, preferred_element_type=jnp.float32).reshape(length, HEADS, ROPE)
    q_rot = rotate(q_raw, cosine[:, None, :], sine[:, None, :]).astype(jnp.bfloat16)
    k_plain = jnp.dot(kv_norm, w_key_plain, preferred_element_type=jnp.float32).astype(jnp.bfloat16).reshape(length, HEADS, NOPE)
    values = jnp.dot(kv_norm, w_value, preferred_element_type=jnp.float32).astype(jnp.bfloat16).reshape(length, HEADS, VDIM)
    k_wide = k_plain.astype(jnp.float32)
    v_wide = values.astype(jnp.float32)
    r_wide = key_rot.astype(jnp.float32)
    scale = (NOPE + ROPE) ** (-0.5)
    blocks = length // TOK_DEV

    def attend(pair):
        q_a, q_b = pair
        score = (jnp.einsum('qhd,khd->hqk', q_a.astype(jnp.float32), k_wide) + jnp.einsum('qhr,kr->hqk', q_b.astype(jnp.float32), r_wide)) * scale
        top = lax.optimization_barrier(jnp.max(score, axis=-1, keepdims=True))
        weight = jnp.exp(score - top)
        total = lax.optimization_barrier(jnp.sum(weight, axis=-1))
        mixed = jnp.einsum('hqk,khd->qhd', weight.astype(jnp.bfloat16).astype(jnp.float32), v_wide)
        return (mixed / jnp.transpose(total)[:, :, None]).astype(jnp.bfloat16)
    attn = lax.map(attend, (q_plain.reshape(blocks, TOK_DEV, HEADS, NOPE), q_rot.reshape(blocks, TOK_DEV, HEADS, ROPE)))
    attn = attn.reshape(length, HEADS * VDIM)
    mid = resid_in.astype(jnp.float32) + jnp.dot(attn, w_output, preferred_element_type=jnp.float32)
    h_norm = normed(mid, ffn_gain).astype(jnp.bfloat16)
    gate = jnp.dot(h_norm, w_gate, preferred_element_type=jnp.float32)
    upper = jnp.dot(h_norm, w_up, preferred_element_type=jnp.float32)
    hidden = (jax.nn.silu(gate) * upper).astype(jnp.bfloat16)
    return (mid + jnp.dot(hidden, w_down, preferred_element_type=jnp.float32)).astype(jnp.bfloat16)
```

```python
import functools

import jax
import jax.numpy as jnp
from jax import lax
from jax.experimental import pallas as pl
from jax.experimental.pallas import tpu as pltpu
from jax.sharding import PartitionSpec as P

NOPE = 128
ROPE = 64
VDIM = 128
MESH = pl.DeviceIdType.MESH


def normed(values, gain):
    wide = values.astype(jnp.float32)
    return wide * lax.rsqrt(jnp.mean(wide * wide, axis=-1, keepdims=True) + 1e-06) * gain


class Plan:
    def __init__(self, sp, tp):
        self.sp, self.tp = sp, tp
        self.z = 4 if sp % 4 == 0 else 1
        self.r = sp // self.z
        self.c = 2 if tp % 2 == 0 else 1
        self.x = tp // self.c

    def sizes(self):
        return {"z": self.z, "r": self.r, "x": self.x, "c": self.c}

    def here(self):
        s, t = lax.axis_index("sp"), lax.axis_index("tp")
        return {"z": s // self.r, "r": lax.rem(s, self.r), "x": t // self.c, "c": lax.rem(t, self.c)}

    def device(self, at):
        return {"sp": at["z"] * self.r + at["r"], "tp": at["x"] * self.c + at["c"]}

    def shifted(self, at, axis, by):
        size = self.sizes()[axis]
        return {**at, axis: lax.rem(at[axis] + (by % size), size)}

    def far(self):
        return (2, 3, 1) if self.z == 4 else ()

    def partner(self, at, m):
        z = at["z"]
        if m == 1:
            z = z + 1 - 2 * lax.rem(z, 2)
        elif m == 2:
            z = lax.rem(z + 2, 4)
        elif m == 3:
            z = 3 - z
        return {**at, "z": z}


def front_body(
    plan,
    heads,
    part,
    ql_ref,
    kvl_ref,
    rk_ref,
    qg_ref,
    kg_ref,
    cos_ref,
    sin_ref,
    gain_ref,
    wqp_hbm,
    wqr_hbm,
    wk_hbm,
    wv_hbm,
    wo_hbm,
    resid_hbm,
    gate_ref,
    up_ref,
    down_ref,
    o_ref,
    mid_ref,
    hn_ref,
    both_ref,
    downs_ref,
    packed,
    attn,
    wqp_ref,
    wqr_ref,
    wk_ref,
    wv_ref,
    wo_ref,
    resid_ref,
    qcat,
    proj_ref,
    outp,
    swap_c,
    swap_s,
    swap_x,
    hidden,
    part_ref,
    got_c,
    sum_c,
    got_x,
    sum_x,
    got_z,
    kz_s,
    kz_r,
    ky_s,
    ky_r,
    kx_s,
    kx_r,
    kc_s,
    kc_r,
    wz_s,
    wz_r,
    wy_s,
    wy_r,
    sc_s,
    sc_r,
    sx_s,
    sx_r,
    hz_s,
    hz_r,
    hx_s,
    hx_r,
    hc_s,
    hc_r,
    fc_s,
    fc_r,
    fx_s,
    fx_r,
    fz_s,
    fz_r,
    local,
):
    here = plan.here()
    nz, nr, nx, nc, tp = plan.z, plan.r, plan.x, plan.c, plan.tp
    far = plan.far()
    z, r, x, c = here["z"], here["r"], here["x"], here["c"]
    latent = wk_ref.shape[0]
    depth, full = gate_ref.shape
    narrow = down_ref.shape[1]
    tok = ql_ref.shape[0]
    share = tok // tp
    sp_here, tp_here = lax.axis_index("sp"), lax.axis_index("tp")
    wide, bf = jnp.float32, jnp.bfloat16
    f32 = wide
    waits = []

    def drain():
        while waits:
            waits.pop().wait_send()

    def peer(axis, by):
        return plan.device(plan.shifted(here, axis, by))

    def zpeer(m):
        return plan.device(plan.partner(here, m))

    def zof(m):
        return plan.partner(here, m)["z"]

    barrier = pltpu.get_barrier_semaphore()
    peers = [zpeer(m) for m in far]
    for axis, size in (("r", nr), ("x", nx), ("c", nc)):
        peers += [peer(axis, k) for k in range(1, size)]
    for to in peers:
        pl.semaphore_signal(barrier, inc=1, device_id=to, device_id_type=MESH)

    loads = [
        (wqp_hbm, wqp_ref),
        (wqr_hbm, wqr_ref),
        (wk_hbm, wk_ref),
        (wv_hbm, wv_ref),
        (wo_hbm, wo_ref),
        (resid_hbm.at[pl.ds(pl.multiple_of(tp_here * share, share), share)], resid_ref),
    ]
    loads = [pltpu.make_async_copy(s, d, local.at[i]) for i, (s, d) in enumerate(loads)]
    for copy in loads:
        copy.start()

    def send(src, dst, device, sem_s, sem_r):
        copy = pltpu.make_async_remote_copy(
            src_ref=src,
            dst_ref=dst,
            send_sem=sem_s,
            recv_sem=sem_r,
            device_id=device,
            device_id_type=MESH,
        )
        copy.start()
        waits.append(copy)
        return copy

    pair = 2 * ROPE
    lane = lax.broadcasted_iota(jnp.int32, (1, pair), 1)
    first = lax.rem(lane, ROPE) < ROPE // 2

    def rotated(v):
        other = jnp.where(first, pltpu.roll(v, pair - ROPE // 2, 1), pltpu.roll(v, ROPE // 2, 1))
        return (v * cos_ref[...] + other * sin_ref[...]).astype(bf)

    def block_of(at):
        return at["z"] * nr + at["r"]

    with jax.named_scope("kvprep"):
        lat = normed(kvl_ref[...], kg_ref[...][None, :]).astype(bf)
        raw = rk_ref[...].astype(f32)
        rot = rotated(jnp.concatenate([raw, raw], axis=0).T)
        for i in range(tp):
            rows = slice(i * share, (i + 1) * share)
            packed[sp_here, i % nc, i // nc, :, :latent] = lat[rows]
            packed[sp_here, i % nc, i // nc, :, latent:] = rot[rows]

    with jax.named_scope("barrier"):
        pl.semaphore_wait(barrier, len(peers))

    kz, ky, kx, kc = {}, {}, {}, {}

    def kv_at(m, j):
        return block_of(plan.shifted(plan.partner(here, m), "r", -j))

    def kv_y(m):
        q = packed.at[kv_at(m, 0), c]
        q = q if m == 0 else q.at[x]
        for j in range(1, nr):
            ky[m, j] = send(q, q, peer("r", j), ky_s.at[m, j], ky_r.at[m, j])

    def kv_x(m, j):
        for l in range(1, nx):
            q = packed.at[kv_at(m, j), c, x]
            kx[m, j, l] = send(q, q, peer("x", l), kx_s.at[m, j, l], kx_r.at[m, j, l])

    def kv_c(m, j):
        for l in range(1, nx):
            if (m, j, l) in kx:
                kx[m, j, l].wait_recv()
        for l in range(1, nc):
            q = packed.at[kv_at(m, j), c]
            kc[m, j, l] = send(q, q, peer("c", l), kc_s.at[m, j, l], kc_r.at[m, j, l])

    own = packed.at[sp_here, c]
    for m in far:
        q = own if m == 1 else own.at[x]
        kz[m] = send(q, q, zpeer(m), kz_s.at[m], kz_r.at[m])
    kv_y(0)

    def window(index):
        return pl.multiple_of(jnp.minimum(index * part, full - part), 128)

    def targets(sp):
        rows = pl.ds(pl.multiple_of(sp * depth, depth), depth)
        if len(downs_ref.shape) == 3:
            downs = downs_ref.at[sp]
        else:
            downs = downs_ref.at[:, pl.ds(pl.multiple_of(sp * narrow, 128), narrow)]
        return [
            both_ref.at[rows, pl.ds(0, part)],
            both_ref.at[rows, pl.ds(part, part)],
            downs,
        ]

    def sources(index):
        lanes = pl.ds(window(index), part)
        return [gate_ref.at[:, lanes], up_ref.at[:, lanes], down_ref.at[lanes, :]]

    over_z, over_r = {}, {}
    streams = []
    mine = []

    for w in range(3):
        for m in far:
            over_z[w, m] = pltpu.make_async_remote_copy(
                src_ref=sources(zof(m))[w],
                dst_ref=targets(sp_here)[w],
                send_sem=wz_s.at[w, m],
                recv_sem=wz_r.at[w, m],
                device_id=zpeer(m),
                device_id_type=MESH,
            )

    inside = lax.rem(z, 3) != 0
    outside = lax.rem(z, 3) == 0

    def spread(w, *ms):
        for m in ms:
            if m in far:
                over_z[w, m].start()

    def spread_if(when, w, *ms):
        @pl.when(when)
        def _():
            spread(w, *ms)

    def forward(w, m):
        dst = targets(kv_at(m, 0))[w]
        src = dst if m else sources(z)[w]
        if m:
            over_z[w, m].wait_recv()
        for j in range(1, nr):
            over_r[w, m, j] = send(src, dst, peer("r", j), wy_s.at[w, m, j], wy_r.at[w, m, j])
            streams.append(waits.pop())

    for w in range(3):
        mine.append(pltpu.make_async_copy(sources(z)[w], targets(sp_here)[w], local.at[8 + w]))
        mine[-1].start()

    early = len(proj_ref.shape) == 3

    def project(sp):
        if early:
            kv = packed[sp, :, :, :, :latent].reshape(tok, latent)
            for i, w_ref in enumerate((wk_ref, wv_ref)):
                out = jnp.dot(kv, w_ref[...], preferred_element_type=f32)
                proj_ref[i, pl.ds(pl.multiple_of(sp * tok, tok), tok), :] = out.astype(bf)

    with jax.named_scope("qprep"):
        qn = normed(ql_ref[...], qg_ref[...][None, :]).astype(bf)
        loads[0].wait()
        loads[1].wait()
        plain = jnp.dot(qn, wqp_ref[...], preferred_element_type=f32).astype(bf)
        turned = jnp.dot(qn, wqr_ref[...], preferred_element_type=f32)
        for h in range(heads):
            p = h // 2 * pair
            both = rotated(turned[:, p : p + pair])
            keep = (lane >= ROPE) if h % 2 else (lane < ROPE)
            qcat[h, :, :NOPE] = plain[:, h * NOPE : (h + 1) * NOPE]
            qcat[h, :, NOPE:] = jnp.where(keep, both.astype(f32), 0.0).astype(bf)

    loads[2].wait()
    loads[3].wait()
    with jax.named_scope("projown"):
        project(sp_here)
    with jax.named_scope("kvz"):
        for m in far:
            kz[m].wait_recv()
            kv_y(m)
            if m == 1:
                kv_c(m, 0)
            else:
                kv_x(m, 0)
    spread(0, *far)
    spread_if(inside, 1, 2, 1)
    spread_if(outside, 1, 3)
    spread_if(inside, 1, 3)
    spread_if(outside, 1, 2, 1)
    near = [(0, j) for j in range(1, nr)] + [(1, 0)][: len(far)]
    rest = [(m, 0) for m in far if m != 1]
    late = [(m, j) for j in range(1, nr) for m in far]

    def landed(keys):
        for m, j in keys:
            for l in range(1, nc):
                kc[m, j, l].wait_recv()
            project(kv_at(m, j))

    with jax.named_scope("kvy"):
        for j in range(1, nr):
            ky[0, j].wait_recv()
            kv_c(0, j)
        for m, j in late:
            ky[m, j].wait_recv()
            kv_x(m, j)
    with jax.named_scope("near"):
        landed(near)
    with jax.named_scope("kvc"):
        for m, j in rest:
            kv_c(m, j)
        with jax.named_scope("kvcl"):
            landed(rest)
    with jax.named_scope("kvlate"):
        for key in late:
            kv_c(*key)
        for w in range(3):
            forward(w, 0)
        landed(late)

    scale = (NOPE + ROPE) ** (-0.5)
    count = plan.sp * tok

    def transposed(left, right):
        return lax.dot_general(
            left, right, (((1,), (1,)), ((), ())), preferred_element_type=f32
        )

    def head(h):
        lanes = pl.ds(pl.multiple_of(h * NOPE, NOPE), NOPE)
        rot = packed[:, :, :, :, latent:].reshape(count, pair)
        if early:
            plain, vals = proj_ref[0, :, lanes], proj_ref[1, :, lanes]
        else:
            kv = packed[:, :, :, :, :latent].reshape(count, latent)
            weights = jnp.concatenate([wk_ref[:, lanes], wv_ref[:, lanes]], axis=1)
            mixed = jnp.dot(kv, weights, preferred_element_type=f32).astype(bf)
            plain, vals = mixed[:, :NOPE], mixed[:, NOPE:]
        score = transposed(qcat[h], jnp.concatenate([plain, rot], axis=1)) * scale
        weight = jnp.exp(score - jnp.max(score, axis=-1, keepdims=True))
        total = jnp.sum(weight, axis=-1, keepdims=True)
        value = jnp.dot(weight.astype(bf), vals, preferred_element_type=f32)
        attn[:, lanes] = (value / total).astype(bf)

    todo = [(w, m) for w in range(2) for m in far]

    def pump(n):
        for _ in range(n):
            if todo:
                forward(*todo.pop(0))

    @pl.loop(0, heads)
    def _(h):
        with jax.named_scope("head"):
            head(h)

    with jax.named_scope("pump0"):
        pump(PUMPS[0])
    with jax.named_scope("outproj"):
        loads[4].wait()
        loads[5].wait()
        term = jnp.dot(attn[...], wo_ref[...], preferred_element_type=f32).astype(bf)
        for i in range(tp):
            outp[i % nc, i // nc] = term[i * share : (i + 1) * share]
    swaps_c = [
        send(
            outp.at[lax.rem(c + l, nc)], swap_c.at[l - 1], peer("c", l), sc_s.at[l], sc_r.at[l]
        )
        for l in range(1, nc)
    ]
    with jax.named_scope("swapc"):
        for copy in swaps_c:
            copy.wait_recv()

    def folded(i):
        total = outp[c, i].astype(f32)
        for l in range(1, nc):
            total += swap_c[l - 1, i].astype(f32)
        return total

    swaps_x = []
    for l in range(1, nx):
        i = lax.rem(x + l, nx)
        swap_s[l - 1] = folded(i).astype(bf)
        swaps_x.append(
            send(swap_s.at[l - 1], swap_x.at[l - 1], peer("x", l), sx_s.at[l], sx_r.at[l])
        )
    mid = resid_ref[...].astype(f32) + folded(x)
    with jax.named_scope("pumpA"):
        pump(PUMPS[1])
    drain()
    with jax.named_scope("swapx"):
        for l, copy in enumerate(swaps_x):
            copy.wait_recv()
            mid += swap_x[l].astype(f32)
    mid_ref[...] = mid
    hn_ref[z, c, x] = (
        mid * lax.rsqrt(jnp.mean(mid * mid, axis=-1, keepdims=True) + 1e-06) * gain_ref[...][None, :]
    ).astype(bf)

    hz, hx, hc = {}, {}, {}
    order = (0,) + tuple(range(1, nz))
    half = z // 2
    origin = (z, z + 1 - 2 * lax.rem(z, 2), 2 - half, 3 - 3 * half)[:nz]
    inner_z = inside

    def hn_z(k, device, at):
        q = hn_ref.at[origin[k], c, x]
        return pltpu.make_async_remote_copy(
            src_ref=q,
            dst_ref=q,
            send_sem=hz_s.at[k, at],
            recv_sem=hz_r.at[at],
            device_id=device,
            device_id_type=MESH,
        )

    def hn_send(copy, when=None):
        @pl.when(inner_z if when is None else when)
        def _():
            copy.start()

        hops.append(copy)

    hops = []

    def hn_x(k):
        q = hn_ref.at[origin[k], c, x]
        for l in range(1, nx):
            hx[k, l] = send(q, q, peer("x", l), hx_s.at[k, l], hx_r.at[k, l])

    def hn_c(k):
        for l in range(1, nx):
            hx[k, l].wait_recv()
        q = hn_ref.at[origin[k], c]
        for l in range(1, nc):
            hc[k, l] = send(q, q, peer("c", l), hc_s.at[k, l], hc_r.at[k, l])

    if nz > 1:
        direct = hn_z(0, zpeer(1), 1)
        direct.start()
        waits.append(direct)
        hn_send(hn_z(0, zpeer(3), 2))
    hn_x(0)
    if nz > 1:
        with jax.named_scope("hn1"):
            hn_z(1, zpeer(1), 1).wait_recv()
            hn_send(hn_z(1, zpeer(3), 3))
            hn_x(1)
        spread_if(inside, 2, 3)
        with jax.named_scope("pumpB"):
            pump(PUMPS[2])
        hn_c(0)
        with jax.named_scope("hn2"):
            hn_z(2, zpeer(1), 2).wait_recv()
            hn_send(hn_z(2, zpeer(1), 2))
            hn_x(2)
        spread_if(outside, 2, 2, 1)
        hn_c(1)
        with jax.named_scope("hn3"):
            hn_z(3, zpeer(1), 3).wait_recv()
            hn_send(hn_z(3, zpeer(1), 3))
            hn_x(3)
        spread_if(inside, 2, 2, 1)
        spread_if(outside, 2, 3)
    else:
        hn_c(0)
    with jax.named_scope("pumpC"):
        pump(9)
    todo += [(2, m) for m in far]
    for k in order[2:]:
        with jax.named_scope(f"hnc{k}"):
            hn_c(k)
    with jax.named_scope("gateup"):
        for w in range(2):
            mine[w].wait()
            for m in (0,) + far:
                for j in range(1, nr):
                    over_r[w, m, j].wait_recv()

    place = z * part
    lanes = lax.broadcasted_iota(jnp.int32, (1, part), 1)
    fresh = lanes >= place - jnp.minimum(place, full - part)

    def inner(k):
        for l in range(1, nc):
            hc[k, l].wait_recv()
        rows = hn_ref[origin[k]].reshape(tp * share, -1)
        both = jnp.dot(rows, both_ref[...], preferred_element_type=f32)
        value = jnp.where(fresh, jax.nn.silu(both[:, :part]) * both[:, part:], 0.0)
        hidden[origin[k]] = value.astype(bf)

    for k in order:
        with jax.named_scope(f"inner{k}"):
            inner(k)
    order = (0,) + far
    pump(PUMPS[3])

    over_c, over_x, back = {}, {}, {}
    group = nr * narrow

    def feed(m):
        if m == 0:
            mine[2].wait()
        for j in range(1, nr):
            over_r[2, m, j].wait_recv()
        rows = hidden[...].reshape(nz * tp * share, part)

        def keep(piece, columns):
            piece = piece.astype(bf).reshape(nz, nc, nx, share, -1)
            for i in range(nc):
                part_ref[m, i, :, :, :, columns] = piece[:, i]

        if len(downs_ref.shape) == 3:
            for i in range(nr):
                piece = jnp.dot(rows, downs_ref[zof(m) * nr + i], preferred_element_type=f32)
                keep(piece, slice(i * narrow, (i + 1) * narrow))
        else:
            columns = pl.ds(pl.multiple_of(zof(m) * group, 128), group)
            keep(jnp.dot(rows, downs_ref[:, columns], preferred_element_type=f32), slice(None))
        for l in range(1, nc):
            over_c[m, l] = send(
                part_ref.at[m, lax.rem(c + l, nc)],
                got_c.at[m, l - 1],
                peer("c", l),
                fc_s.at[m, l],
                fc_r.at[m, l],
            )

    def fold_c(m):
        for l in range(1, nc):
            over_c[m, l].wait_recv()
        for k in range(1, nx + 1):
            i = lax.rem(x + k, nx)
            total = part_ref[m, c, :, i].astype(f32)
            for l in range(1, nc):
                total += got_c[m, l - 1, :, i].astype(f32)
            sum_c[m, i] = total.astype(bf)
            if k < nx:
                over_x[m, k] = send(
                    sum_c.at[m, i], got_x.at[m, k - 1], peer("x", k), fx_s.at[m, k], fx_r.at[m, k]
                )

    def columns_of(m):
        return pl.ds(pl.multiple_of(zof(m) * group, 128), group)

    def fold_x(m):
        for k in range(1, nx):
            over_x[m, k].wait_recv()
        for p in far + (0,):
            total = sum_c[m, x, zof(p)].astype(f32)
            for k in range(1, nx):
                total += got_x[m, k - 1, zof(p)].astype(f32)
            if p == 0:
                mid_ref[:, columns_of(m)] += total
                continue
            sum_x[m, p] = total.astype(bf)
            there = m ^ p
            back[there, p] = send(
                sum_x.at[m, p], got_z.at[there, p], zpeer(p), fz_s.at[m, p], fz_r.at[there, p]
            )

    def close(m):
        total = mid_ref[:, columns_of(m)]
        for p in far:
            back[m, p].wait_recv()
            total += got_z[m, p].astype(f32)
        o_ref[:, columns_of(m)] = total.astype(bf)

    plain = ((feed, 0), (pump, 1), (fold_c, 0), (pump, 1), (feed, 1), (fold_c, 1), (pump, 1))
    plain += ((fold_x, 0), (feed, 2), (fold_c, 2), (fold_x, 1), (feed, 3), (fold_c, 3))
    def settle(i):
        for copy in over_z.values():
            copy.wait_send()
        for copy in hops:

            @pl.when(inner_z)
            def _():
                copy.wait_send()

        last = {id(copy) for copy in back.values()}
        held = streams + [copy for copy in waits if id(copy) not in last]
        waits[:] = [copy for copy in waits if id(copy) in last]
        for copy in held:
            copy.wait_send()

    plain += ((fold_x, 2), (settle, 0), (fold_x, 3), (close, 0), (close, 1), (close, 2), (close, 3))
    for stage, i in plain:
        with jax.named_scope(f"{stage.__name__}{i}"):
            if stage is pump:
                pump(i)
            elif i < len(order):
                stage(order[i])
    drain()


PUMPS = (1, 2, 3, 0)


def front(plan, heads, part, args):
    nz, nr, nx, nc, tp = plan.z, plan.r, plan.x, plan.c, plan.tp
    ql, kvl = args[0], args[1]
    wqp, wqr, wk, wv, wo, resid, gate, up, down = args[8:]
    tok, width = resid.shape
    share = tok // tp
    dma = pltpu.SemaphoreType.DMA
    vmem = pl.BlockSpec(memory_space=pltpu.VMEM)
    hbm = pl.BlockSpec(memory_space=pl.ANY)
    bf = jnp.bfloat16
    narrow = down.shape[1]
    group = nr * narrow
    downs = (part, plan.sp * narrow) if narrow % 128 == 0 else (plan.sp, part, narrow)
    proj = (2, plan.sp * tok, heads * NOPE)
    proj = pltpu.VMEM(proj if 4 * proj[1] * proj[2] < 2**23 + 1 else (8, 128), bf)
    more_c, more_x = max(nc - 1, 1), max(nx - 1, 1)
    sizes = [(nz,), (nz, nr), (nz, nr, nx), (nz, nr, nc), (3, nz), (3, nz, nr), (nc,), (nx,)]
    sems = [dma(size) for size in sizes for _ in range(2)]
    sems += [dma((2 * nz, 4)), dma((4,))]
    sizes = [(nz, nx), (nz, nc), (nz, nc), (nz, nx), (nz, nz)]
    sems += [dma(size) for size in sizes for _ in range(2)]
    return pl.pallas_call(
        functools.partial(front_body, plan, heads, part),
        out_shape=jax.ShapeDtypeStruct((share, width), bf),
        in_specs=[vmem] * 8 + [hbm] * 9,
        out_specs=vmem,
        scratch_shapes=[
            pltpu.VMEM((share, width), jnp.float32),
            pltpu.VMEM((nz, nc, nx, share, width), bf),
            pltpu.VMEM((plan.sp * gate.shape[0], 2 * part), bf),
            pltpu.VMEM(downs, bf),
            pltpu.VMEM((plan.sp, nc, nx, share, kvl.shape[1] + 2 * ROPE), bf),
            pltpu.VMEM((tok, heads * VDIM), bf),
            pltpu.VMEM(wqp.shape, bf),
            pltpu.VMEM(wqr.shape, bf),
            pltpu.VMEM(wk.shape, bf),
            pltpu.VMEM(wv.shape, bf),
            pltpu.VMEM(wo.shape, bf),
            pltpu.VMEM((share, width), bf),
            pltpu.VMEM((heads, tok, NOPE + 2 * ROPE), bf),
            proj,
            pltpu.VMEM((nc, nx, share, width), bf),
            pltpu.VMEM((more_c, nx, share, width), bf),
            pltpu.VMEM((more_x, share, width), bf),
            pltpu.VMEM((more_x, share, width), bf),
            pltpu.VMEM((nz, tp * share, part), bf),
            pltpu.VMEM((nz, nc, nz, nx, share, group), bf),
            pltpu.VMEM((nz, more_c, nz, nx, share, group), bf),
            pltpu.VMEM((nz, nx, nz, share, group), bf),
            pltpu.VMEM((nz, more_x, nz, share, group), bf),
            pltpu.VMEM((nz, nz, share, group), bf),
            pltpu.VMEM((nz, nz, share, group), bf),
            *sems,
            dma((11,)),
        ],
        compiler_params=pltpu.CompilerParams(
            collective_id=1, has_side_effects=True, vmem_limit_bytes=62 * 1024 * 1024
        ),
    )(*args)


def shards(
    plan,
    resid_in,
    query_latent,
    kv_latent,
    rotary_key,
    query_gain,
    kv_gain,
    w_query_plain,
    w_query_rotary,
    w_key_plain,
    w_value,
    w_output,
    ffn_gain,
    w_gate,
    w_up,
    w_down,
):
    tok = resid_in.shape[0]
    heads_dev = w_query_plain.shape[1] // NOPE
    hidden_dev = w_gate.shape[1]
    part = min(-(-hidden_dev // (plan.z * 128)) * 128, hidden_dev)

    offset = lax.axis_index("sp") * tok
    position = (offset + jnp.arange(tok, dtype=jnp.int32)).astype(jnp.float32)
    lane = lax.broadcasted_iota(jnp.int32, (1, 2 * ROPE), 1)
    index = lax.rem(lane, ROPE // 2) * 2
    freq = 10000.0 ** (-index.astype(jnp.float32) / ROPE)
    angle = position[:, None] * freq
    sign = jnp.where(lax.rem(lane, ROPE) < ROPE // 2, -1.0, 1.0)
    return front(
        plan,
        heads_dev,
        part,
        (
            query_latent,
            kv_latent,
            jnp.transpose(rotary_key),
            query_gain,
            kv_gain,
            jnp.cos(angle),
            jnp.sin(angle) * sign,
            ffn_gain,
            w_query_plain,
            w_query_rotary,
            w_key_plain,
            w_value,
            w_output,
            resid_in,
            w_gate,
            w_up,
            w_down,
        ),
    )


def solution(mesh):
    plan = Plan(mesh.shape["sp"], mesh.shape["tp"])
    return jax.shard_map(
        functools.partial(shards, plan),
        mesh=mesh,
        in_specs=(
            P("sp", None),
            P("sp", None),
            P("sp", None),
            P("sp", None),
            P(),
            P(),
            P(None, "tp"),
            P(None, "tp"),
            P(None, "tp"),
            P(None, "tp"),
            P("tp", None),
            P(),
            P("sp", "tp"),
            P("sp", "tp"),
            P("tp", "sp"),
        ),
        out_specs=P(("sp", "tp"), None),
        check_vma=False,
    )
```

```python
import functools

import jax
import jax.numpy as jnp
from jax import lax
from jax.experimental import pallas as pl
from jax.experimental.pallas import tpu as pltpu
from jax.sharding import PartitionSpec as P

NOPE = 128
ROPE = 64
VDIM = 128
MESH = pl.DeviceIdType.MESH


def normed(values, gain):
    wide = values.astype(jnp.float32)
    return wide * lax.rsqrt(jnp.mean(wide * wide, axis=-1, keepdims=True) + 1e-06) * gain


class Plan:
    def __init__(self, sp, tp):
        self.sp, self.tp = sp, tp
        self.z = 4 if sp % 4 == 0 else 1
        self.r = sp // self.z
        self.c = 2 if tp % 2 == 0 else 1
        self.x = tp // self.c

    def sizes(self):
        return {"z": self.z, "r": self.r, "x": self.x, "c": self.c}

    def here(self):
        s, t = lax.axis_index("sp"), lax.axis_index("tp")
        return {"z": s // self.r, "r": lax.rem(s, self.r), "x": t // self.c, "c": lax.rem(t, self.c)}

    def device(self, at):
        return {"sp": at["z"] * self.r + at["r"], "tp": at["x"] * self.c + at["c"]}

    def shifted(self, at, axis, by):
        size = self.sizes()[axis]
        return {**at, axis: lax.rem(at[axis] + (by % size), size)}

    def far(self):
        return (2, 3, 1) if self.z == 4 else ()

    def partner(self, at, m):
        z = at["z"]
        if m == 1:
            z = z + 1 - 2 * lax.rem(z, 2)
        elif m == 2:
            z = lax.rem(z + 2, 4)
        elif m == 3:
            z = 3 - z
        return {**at, "z": z}


def front_body(
    plan,
    heads,
    part,
    ql_hbm,
    kvl_hbm,
    rk_hbm,
    qg_hbm,
    kg_hbm,
    cos_hbm,
    sin_hbm,
    gain_hbm,
    wqp_hbm,
    wqr_hbm,
    wk_hbm,
    wv_hbm,
    wo_hbm,
    resid_hbm,
    gate_ref,
    up_ref,
    down_ref,
    o_ref,
    mid_ref,
    hn_ref,
    both_ref,
    downs_ref,
    packed,
    attn,
    ql_ref,
    kvl_ref,
    rk_ref,
    qg_ref,
    kg_ref,
    cos_ref,
    sin_ref,
    gain_ref,
    wqp_ref,
    wqr_ref,
    wk_ref,
    wv_ref,
    wo_ref,
    resid_ref,
    qcat,
    proj_ref,
    outp,
    swap_c,
    swap_s,
    swap_x,
    hidden,
    part_ref,
    got_c,
    sum_c,
    got_x,
    sum_z,
    got_z,
    done,
    kz_s,
    kz_r,
    ky_s,
    ky_r,
    kx_s,
    kx_r,
    kc_s,
    kc_r,
    wz_s,
    wz_r,
    wy_s,
    wy_r,
    sc_s,
    sc_r,
    sx_s,
    sx_r,
    hz_s,
    hz_r,
    hx_s,
    hx_r,
    hc_s,
    hc_r,
    fc_s,
    fc_r,
    fx_s,
    fx_r,
    fz_s,
    fz_r,
    local,
):
    here = plan.here()
    nz, nr, nx, nc, tp = plan.z, plan.r, plan.x, plan.c, plan.tp
    far = plan.far()
    z, r, x, c = here["z"], here["r"], here["x"], here["c"]
    latent = wk_ref.shape[0]
    depth, full = gate_ref.shape
    narrow = down_ref.shape[1]
    tok = ql_ref.shape[0]
    share = tok // tp
    sp_here, tp_here = lax.axis_index("sp"), lax.axis_index("tp")
    wide, bf = jnp.float32, jnp.bfloat16
    f32 = wide
    waits = []

    def drain():
        while waits:
            waits.pop().wait_send()

    def peer(axis, by):
        return plan.device(plan.shifted(here, axis, by))

    def zpeer(m):
        return plan.device(plan.partner(here, m))

    def zof(m):
        return plan.partner(here, m)["z"]

    barrier = pltpu.get_barrier_semaphore()
    peers = [zpeer(m) for m in far]
    for axis, size in (("r", nr), ("x", nx), ("c", nc)):
        peers += [peer(axis, k) for k in range(1, size)]
    for to in peers:
        pl.semaphore_signal(barrier, inc=1, device_id=to, device_id_type=MESH)

    smalls = [
        (kvl_hbm, kvl_ref),
        (kg_hbm, kg_ref),
        (rk_hbm, rk_ref),
        (cos_hbm, cos_ref),
        (sin_hbm, sin_ref),
        (ql_hbm, ql_ref),
        (qg_hbm, qg_ref),
        (gain_hbm, gain_ref),
    ]
    base = 11 + nz
    smalls = [pltpu.make_async_copy(s, d, local.at[base + i]) for i, (s, d) in enumerate(smalls)]
    for copy in smalls:
        copy.start()
    loads = [
        (wqp_hbm, wqp_ref),
        (wqr_hbm, wqr_ref),
        (wk_hbm, wk_ref),
        (wv_hbm, wv_ref),
        (wo_hbm, wo_ref),
        (resid_hbm.at[pl.ds(pl.multiple_of(tp_here * share, share), share)], resid_ref),
    ]
    loads = [pltpu.make_async_copy(s, d, local.at[i]) for i, (s, d) in enumerate(loads)]
    for copy in loads:
        copy.start()

    def send(src, dst, device, sem_s, sem_r):
        copy = pltpu.make_async_remote_copy(
            src_ref=src,
            dst_ref=dst,
            send_sem=sem_s,
            recv_sem=sem_r,
            device_id=device,
            device_id_type=MESH,
        )
        copy.start()
        waits.append(copy)
        return copy

    pair = 2 * ROPE
    lane = lax.broadcasted_iota(jnp.int32, (1, pair), 1)
    first = lax.rem(lane, ROPE) < ROPE // 2

    def rotated(v):
        other = jnp.where(first, pltpu.roll(v, pair - ROPE // 2, 1), pltpu.roll(v, ROPE // 2, 1))
        return (v * cos_ref[...] + other * sin_ref[...]).astype(bf)

    def block_of(at):
        return at["z"] * nr + at["r"]

    for copy in smalls[:5]:
        copy.wait()
    with jax.named_scope("kvprep"):
        lat = normed(kvl_ref[...], kg_ref[...][None, :]).astype(bf)
        raw = rk_ref[...].astype(f32)
        rot = rotated(jnp.concatenate([raw, raw], axis=0).T)
        for i in range(tp):
            rows = slice(i * share, (i + 1) * share)
            packed[sp_here, i % nc, i // nc, :, :latent] = lat[rows]
            packed[sp_here, i % nc, i // nc, :, latent:] = rot[rows]

    with jax.named_scope("barrier"):
        pl.semaphore_wait(barrier, len(peers))

    kz, ky, kx, kc = {}, {}, {}, {}

    def kv_at(m, j):
        return block_of(plan.shifted(plan.partner(here, m), "r", -j))

    def kv_y(m):
        q = packed.at[kv_at(m, 0), c]
        q = q if m == 0 else q.at[x]
        for j in range(1, nr):
            ky[m, j] = send(q, q, peer("r", j), ky_s.at[m, j - 1], ky_r.at[m, j - 1])

    def kv_x(m, j):
        for l in range(1, nx):
            q = packed.at[kv_at(m, j), c, x]
            kx[m, j, l] = send(q, q, peer("x", l), kx_s.at[m, j, l - 1], kx_r.at[m, j, l - 1])

    def kv_c(m, j):
        for l in range(1, nx):
            if (m, j, l) in kx:
                kx[m, j, l].wait_recv()
        for l in range(1, nc):
            q = packed.at[kv_at(m, j), c]
            kc[m, j, l] = send(q, q, peer("c", l), kc_s.at[m, j, l - 1], kc_r.at[m, j, l - 1])

    own = packed.at[sp_here, c]
    for m in far:
        q = own if m == 1 else own.at[x]
        kz[m] = send(q, q, zpeer(m), kz_s.at[m], kz_r.at[m])
    kv_y(0)

    def window(index):
        return pl.multiple_of(jnp.minimum(index * part, full - part), 128)

    def targets(sp):
        rows = pl.ds(pl.multiple_of(sp * depth, depth), depth)
        if len(downs_ref.shape) == 3:
            downs = downs_ref.at[sp]
        else:
            downs = downs_ref.at[:, pl.ds(pl.multiple_of(sp * narrow, 128), narrow)]
        return [
            both_ref.at[rows, pl.ds(0, part)],
            both_ref.at[rows, pl.ds(part, part)],
            downs,
        ]

    def sources(index):
        lanes = pl.ds(window(index), part)
        return [gate_ref.at[:, lanes], up_ref.at[:, lanes], down_ref.at[lanes, :]]

    over_z, over_r = {}, {}
    streams = []
    mine = []

    for w in range(3):
        for m in far:
            over_z[w, m] = pltpu.make_async_remote_copy(
                src_ref=sources(zof(m))[w],
                dst_ref=targets(sp_here)[w],
                send_sem=wz_s.at[w, m],
                recv_sem=wz_r.at[w, m],
                device_id=zpeer(m),
                device_id_type=MESH,
            )

    inside = lax.rem(z, 3) != 0
    outside = lax.rem(z, 3) == 0

    def spread(w, *ms):
        for m in ms:
            if m in far:
                over_z[w, m].start()

    def spread_if(when, w, *ms):
        @pl.when(when)
        def _():
            spread(w, *ms)

    def arrange(w, m):
        dst = targets(kv_at(m, 0))[w]
        src = dst if m else sources(z)[w]
        for j in range(1, nr):
            over_r[w, m, j] = pltpu.make_async_remote_copy(
                src_ref=src,
                dst_ref=dst,
                send_sem=wy_s.at[w, m, j - 1],
                recv_sem=wy_r.at[w, m, j - 1],
                device_id=peer("r", j),
                device_id_type=MESH,
            )
            streams.append(over_r[w, m, j])

    def go(w, m):
        if m:
            over_z[w, m].wait_recv()
        for j in range(1, nr):
            over_r[w, m, j].start()

    def forward(w, m):
        arrange(w, m)
        go(w, m)

    for w in range(3):
        for m in far:
            over_z[w, m] = pltpu.make_async_remote_copy(
                src_ref=sources(zof(m))[w],
                dst_ref=targets(sp_here)[w],
                send_sem=wz_s.at[w, m],
                recv_sem=wz_r.at[w, m],
                device_id=zpeer(m),
                device_id_type=MESH,
            )

    inside = lax.rem(z, 3) != 0
    outside = lax.rem(z, 3) == 0

    def spread(w, *ms):
        for m in ms:
            if m in far:
                over_z[w, m].start()

    def spread_if(when, w, *ms):
        @pl.when(when)
        def _():
            spread(w, *ms)

    def forward(w, m):
        dst = targets(kv_at(m, 0))[w]
        src = dst if m else sources(z)[w]
        if m:
            over_z[w, m].wait_recv()
        for j in range(1, nr):
            over_r[w, m, j] = send(src, dst, peer("r", j), wy_s.at[w, m, j - 1], wy_r.at[w, m, j - 1])
            streams.append(waits.pop())

    for w in range(3):
        mine.append(pltpu.make_async_copy(sources(z)[w], targets(sp_here)[w], local.at[8 + w]))
        mine[-1].start()

    early = len(proj_ref.shape) == 3

    def project(sp):
        if early:
            kv = packed[sp, :, :, :, :latent].reshape(tok, latent)
            for i, w_ref in enumerate((wk_ref, wv_ref)):
                out = jnp.dot(kv, w_ref[...], preferred_element_type=f32)
                proj_ref[i, pl.ds(pl.multiple_of(sp * tok, tok), tok), :] = out.astype(bf)

    with jax.named_scope("qprep"):
        for copy in smalls[5:]:
            copy.wait()
        qn = normed(ql_ref[...], qg_ref[...][None, :]).astype(bf)
        loads[0].wait()
        loads[1].wait()
        plain = jnp.dot(qn, wqp_ref[...], preferred_element_type=f32).astype(bf)
        turned = jnp.dot(qn, wqr_ref[...], preferred_element_type=f32)
        for h in range(heads):
            p = h // 2 * pair
            both = rotated(turned[:, p : p + pair])
            keep = (lane >= ROPE) if h % 2 else (lane < ROPE)
            qcat[h, :, :NOPE] = plain[:, h * NOPE : (h + 1) * NOPE]
            qcat[h, :, NOPE:] = jnp.where(keep, both.astype(f32), 0.0).astype(bf)

    loads[2].wait()
    loads[3].wait()
    with jax.named_scope("projown"):
        project(sp_here)
    with jax.named_scope("kvz"):
        for m in far:
            kz[m].wait_recv()
            kv_y(m)
            if m == 1:
                kv_c(m, 0)
            else:
                kv_x(m, 0)
    spread(0, *far)
    spread_if(inside, 1, 2, 1)
    spread_if(outside, 1, 3, 1)
    near = [(0, j) for j in range(1, nr)] + [(1, 0)][: len(far)]
    rest = [(m, 0) for m in far if m != 1]
    late = [(m, j) for j in range(1, nr) for m in far]

    def landed(keys):
        for m, j in keys:
            for l in range(1, nc):
                kc[m, j, l].wait_recv()
            project(kv_at(m, j))

    with jax.named_scope("kvy"):
        for j in range(1, nr):
            ky[0, j].wait_recv()
            kv_c(0, j)
        for m, j in late:
            ky[m, j].wait_recv()
            kv_x(m, j)
    with jax.named_scope("near"):
        landed(near)
    with jax.named_scope("kvc"):
        for m, j in rest:
            kv_c(m, j)
        with jax.named_scope("kvcl"):
            landed(rest)
    with jax.named_scope("kvlate"):
        for key in late:
            kv_c(*key)
        for w in range(2):
            forward(w, 0)
        landed(late)

    scale = (NOPE + ROPE) ** (-0.5)
    count = plan.sp * tok

    def transposed(left, right):
        return lax.dot_general(
            left, right, (((1,), (1,)), ((), ())), preferred_element_type=f32
        )

    def head(h):
        lanes = pl.ds(pl.multiple_of(h * NOPE, NOPE), NOPE)
        rot = packed[:, :, :, :, latent:].reshape(count, pair)
        if early:
            plain, vals = proj_ref[0, :, lanes], proj_ref[1, :, lanes]
        else:
            kv = packed[:, :, :, :, :latent].reshape(count, latent)
            weights = jnp.concatenate([wk_ref[:, lanes], wv_ref[:, lanes]], axis=1)
            mixed = jnp.dot(kv, weights, preferred_element_type=f32).astype(bf)
            plain, vals = mixed[:, :NOPE], mixed[:, NOPE:]
        score = transposed(qcat[h], jnp.concatenate([plain, rot], axis=1)) * scale
        weight = jnp.exp(score - jnp.max(score, axis=-1, keepdims=True))
        total = jnp.sum(weight, axis=-1, keepdims=True)
        value = jnp.dot(weight.astype(bf), vals, preferred_element_type=f32)
        attn[:, lanes] = (value / total).astype(bf)

    todo = [(0, m) for m in far]

    def pump(n):
        for _ in range(n):
            if todo:
                forward(*todo.pop(0))

    @pl.loop(0, heads)
    def _(h):
        with jax.named_scope("head"):
            head(h)

    with jax.named_scope("pump0"):
        pump(PUMPS[0])
    with jax.named_scope("outproj"):
        loads[4].wait()
        loads[5].wait()
        term = jnp.dot(attn[...], wo_ref[...], preferred_element_type=f32).astype(bf)
        for i in range(tp):
            outp[i % nc, i // nc] = term[i * share : (i + 1) * share]
    swaps_c = [
        send(
            outp.at[lax.rem(c + l, nc)], swap_c.at[l - 1], peer("c", l), sc_s.at[l - 1], sc_r.at[l - 1]
        )
        for l in range(1, nc)
    ]
    with jax.named_scope("swapc"):
        for copy in swaps_c:
            copy.wait_recv()

    def folded(i):
        total = outp[c, i].astype(f32)
        for l in range(1, nc):
            total += swap_c[l - 1, i].astype(f32)
        return total

    swaps_x = []
    for l in range(1, nx):
        i = lax.rem(x + l, nx)
        swap_s[l - 1] = folded(i).astype(bf)
        swaps_x.append(
            send(swap_s.at[l - 1], swap_x.at[l - 1], peer("x", l), sx_s.at[l - 1], sx_r.at[l - 1])
        )
    mid = resid_ref[...].astype(f32) + folded(x)
    with jax.named_scope("pumpA"):
        pump(PUMPS[1])
    drain()
    with jax.named_scope("swapx"):
        for l, copy in enumerate(swaps_x):
            copy.wait_recv()
            mid += swap_x[l].astype(f32)
    mid_ref[...] = mid
    hn_ref[z, c, x] = (
        mid * lax.rsqrt(jnp.mean(mid * mid, axis=-1, keepdims=True) + 1e-06) * gain_ref[...][None, :]
    ).astype(bf)

    hz, hx, hc = {}, {}, {}
    order = (0,) + tuple(range(1, nz))
    half = z // 2
    origin = (z, z + 1 - 2 * lax.rem(z, 2), 2 - half, 3 - 3 * half)[:nz]
    inner_z = inside

    def hn_z(k, device, at):
        q = hn_ref.at[origin[k], c, x]
        return pltpu.make_async_remote_copy(
            src_ref=q,
            dst_ref=q,
            send_sem=hz_s.at[{(0, 1): 0, (0, 2): 1, (1, 3): 2, (2, 2): 3, (3, 3): 4}.get((k, at), 0)],
            recv_sem=hz_r.at[at],
            device_id=device,
            device_id_type=MESH,
        )

    def hn_send(copy, when=None):
        @pl.when(inner_z if when is None else when)
        def _():
            copy.start()

        hops.append(copy)

    hops = []

    def hn_x(k):
        q = hn_ref.at[origin[k], c, x]
        for l in range(1, nx):
            hx[k, l] = send(q, q, peer("x", l), hx_s.at[k, l - 1], hx_r.at[k, l - 1])

    for k in order:
        q = hn_ref.at[origin[k], c]
        for l in range(1, nc):
            hc[k, l] = pltpu.make_async_remote_copy(
                src_ref=q,
                dst_ref=q,
                send_sem=hc_s.at[k, l - 1],
                recv_sem=hc_r.at[k, l - 1],
                device_id=peer("c", l),
                device_id_type=MESH,
            )
            waits.append(hc[k, l])

    def hn_c(k):
        for l in range(1, nx):
            hx[k, l].wait_recv()
        for l in range(1, nc):
            hc[k, l].start()

    place = z * part
    lanes = lax.broadcasted_iota(jnp.int32, (1, part), 1)
    fresh = lanes >= place - jnp.minimum(place, full - part)

    def inner(k):
        for l in range(1, nc):
            hc[k, l].wait_recv()
        rows = hn_ref[origin[k]].reshape(tp * share, -1)
        both = jnp.dot(rows, both_ref[...], preferred_element_type=f32)
        value = jnp.where(fresh, jax.nn.silu(both[:, :part]) * both[:, part:], 0.0)
        hidden[origin[k]] = value.astype(bf)

    def ready():
        for w in range(2):
            mine[w].wait()
            for m in (0,) + far:
                for j in range(1, nr):
                    over_r[w, m, j].wait_recv()

    for m in far:
        arrange(1, m)

    def ups(when, *ms):
        @pl.when(when)
        def _():
            for m in ms:
                go(1, m)

    if nz > 1:
        direct = hn_z(0, zpeer(1), 1)
        direct.start()
        waits.append(direct)
        hn_send(hn_z(0, zpeer(3), 2))
    hn_x(0)
    if nz > 1:
        with jax.named_scope("upsout"):
            ups(outside, 2, 1, 3)
            ups(inside, 1)
    forward(2, 0)
    if nz > 1:
        with jax.named_scope("hn1"):
            hn_z(1, zpeer(1), 1).wait_recv()
            hn_send(hn_z(1, zpeer(3), 3))
            hn_x(1)
        spread_if(outside, 1, 2)
        spread_if(outside, 2, 1)
        spread_if(inside, 1, 3)
        with jax.named_scope("hnc0"):
            hn_c(0)
        with jax.named_scope("hn2"):
            hn_z(2, zpeer(1), 2).wait_recv()
            hn_send(hn_z(2, zpeer(1), 2))
            hn_x(2)
        with jax.named_scope("upsin2"):
            ups(inside, 2)
        with jax.named_scope("hnc1"):
            hn_c(1)
        with jax.named_scope("hn3"):
            hn_z(3, zpeer(1), 3).wait_recv()
            hn_send(hn_z(3, zpeer(1), 3))
            hn_x(3)
        spread_if(outside, 2, 2, 3)
        spread_if(inside, 2, 3)
        with jax.named_scope("upsin3"):
            ups(inside, 3)
        spread_if(inside, 2, 1, 2)
    else:
        hn_c(0)

    group = nr * narrow
    halves = 2 if nz > 1 else 1
    deep = nz // halves
    inside_i = jnp.minimum(lax.rem(z, 3), 1)
    groups = origin
    sender = (0,) + ((1, 2 + inside_i, 3 - inside_i) if nz > 1 else ())
    bases = (2 * half, 2 - 2 * half)[:halves] if nz > 1 else (0,)
    landing = {1: ((1, 0, 2, 3),) * 2, 2: ((3, 2, 0, 1), (2, 3, 1, 0)), 3: ((3, 2, 1, 0), (2, 3, 0, 1))}
    away = []
    over_c, over_x, down_r, back = {}, {}, {}, {}

    def remote(src, dst, device, sem_s, sem_r):
        return pltpu.make_async_remote_copy(
            src_ref=src,
            dst_ref=dst,
            send_sem=sem_s,
            recv_sem=sem_r,
            device_id=device,
            device_id_type=MESH,
        )

    def columns_of(i):
        return pl.ds(pl.multiple_of(groups[i] * group, 128), group)

    def down(i):
        dst = targets(groups[i] * nr + r)[2]
        m = sender[i]
        remote(dst, dst, zpeer(1), wz_s.at[2, m], wz_r.at[2, m]).wait_recv()
        for j in range(1, nr):
            down_r[i, j] = send(dst, dst, peer("r", j), wy_s.at[2, m, j - 1], wy_r.at[2, m, j - 1])

    fed = set()

    def feed(i, f):
        if i not in fed:
            fed.add(i)
            if i == 0:
                mine[2].wait()
            for j in range(1, nr):
                (down_r[i, j] if i else over_r[2, 0, j]).wait_recv()
        rows = hidden[pl.ds(bases[f], deep)].reshape(deep * tp * share, part)

        def keep(piece, columns):
            piece = piece.astype(bf).reshape(deep, nc, nx, share, -1)
            for k in range(nc):
                part_ref[i, f, k, :, :, :, columns] = piece[:, k]

        if len(downs_ref.shape) == 3:
            for k in range(nr):
                piece = jnp.dot(rows, downs_ref[groups[i] * nr + k], preferred_element_type=f32)
                keep(piece, slice(k * narrow, (k + 1) * narrow))
        else:
            keep(jnp.dot(rows, downs_ref[:, columns_of(i)], preferred_element_type=f32), slice(None))
        for l in range(1, nc):
            over_c[i, f, l] = send(
                part_ref.at[i, f, lax.rem(c + l, nc)],
                got_c.at[i, f, l - 1],
                peer("c", l),
                fc_s.at[i, f, l - 1],
                fc_r.at[i, f, l - 1],
            )

    def fold_c(i, f):
        for l in range(1, nc):
            over_c[i, f, l].wait_recv()
        for k in range(1, nx + 1):
            to = lax.rem(x + k, nx)
            total = part_ref[i, f, c, :, to].astype(f32)
            for l in range(1, nc):
                total += got_c[i, f, l - 1, :, to].astype(f32)
            sum_c[i, f, to] = total.astype(bf)
            if k < nx:
                over_x[i, f, k] = send(
                    sum_c.at[i, f, to],
                    got_x.at[i, f, k - 1],
                    peer("x", k),
                    fx_s.at[i, f, k - 1],
                    fx_r.at[i, f, k - 1],
                )

    def fold_x(i, f):
        for k in range(1, nx):
            over_x[i, f, k].wait_recv()

        def total(q):
            value = sum_c[i, f, x, q].astype(f32)
            for k in range(1, nx):
                value += got_x[i, f, k - 1, q].astype(f32)
            return value

        def ship(m, q):
            at, to = (table[i] for table in landing[m])
            k = at + inside_i * (to - at)
            sum_z[i, m - 1] = total(q).astype(bf)
            back[i, m] = send(
                sum_z.at[i, m - 1],
                got_z.at[k, m - 1],
                zpeer(m),
                fz_s.at[i, m - 1],
                fz_r.at[k, m - 1],
            )

        if f == 0:
            if nz > 1:
                ship(1, 1 - lax.rem(z, 2))
            mid_ref[:, columns_of(i)] += total(lax.rem(z, deep))
        else:
            for m in (2, 3):
                ship(m, plan.partner(here, m)["z"] - bases[1])

    def close(i):
        total = mid_ref[:, columns_of(i)]
        if nz > 1:
            for m in far:
                q = got_z.at[i, m - 1]
                remote(q, q, zpeer(m), fz_s.at[i, m - 1], fz_r.at[i, m - 1]).wait_recv()
                total += got_z[i, m - 1].astype(f32)
        done[:, columns_of(i)] = total.astype(bf)
        away.append(pltpu.make_async_copy(done.at[:, columns_of(i)], o_ref.at[:, columns_of(i)], local.at[11 + i]))
        away[-1].start()

    def settle(i):
        for copy in over_z.values():
            copy.wait_send()
        for copy in hops:

            @pl.when(inner_z)
            def _():
                copy.wait_send()

        for copy in streams:
            copy.wait_send()
        early_ids = {id(copy) for copy in settled}
        waits[:] = [copy for copy in waits if id(copy) not in early_ids]
        for copy in settled:
            copy.wait_send()

    def step(stage, *key):
        if key[0] < nz and (len(key) < 2 or key[1] < halves):
            with jax.named_scope(stage.__name__ + "_".join(map(str, key))):
                stage(*key)

    with jax.named_scope("gateup"):
        ready()
    step(inner, 0)
    step(inner, 1)
    step(feed, 0, 0)
    if nz > 1:
        with jax.named_scope("hnc2"):
            hn_c(2)
    step(fold_c, 0, 0)
    if nz > 1:
        with jax.named_scope("hnc3"):
            hn_c(3)
    step(inner, 2)
    step(down, 1)
    step(inner, 3)
    step(feed, 0, 1)
    step(fold_c, 0, 1)
    settled = list(waits)
    step(fold_x, 0, 0)
    step(down, 2)
    step(feed, 1, 0)
    step(feed, 1, 1)
    step(fold_c, 1, 0)
    step(fold_c, 1, 1)
    step(fold_x, 0, 1)
    step(down, 3)
    step(feed, 2, 0)
    step(feed, 2, 1)
    step(fold_c, 2, 0)
    step(fold_c, 2, 1)
    step(fold_x, 1, 0)
    step(fold_x, 1, 1)
    step(settle, 0)
    step(feed, 3, 1)
    step(feed, 3, 0)
    step(fold_c, 3, 1)
    step(fold_c, 3, 0)
    step(fold_x, 2, 0)
    step(fold_x, 2, 1)
    step(fold_x, 3, 1)
    step(fold_x, 3, 0)
    for i in range(4):
        step(close, i)
    drain()
    for copy in away:
        copy.wait()


PUMPS = (1, 2)


def front(plan, heads, part, args):
    nz, nr, nx, nc, tp = plan.z, plan.r, plan.x, plan.c, plan.tp
    ql, kvl = args[0], args[1]
    wqp, wqr, wk, wv, wo, resid, gate, up, down = args[8:]
    tok, width = resid.shape
    share = tok // tp
    dma = pltpu.SemaphoreType.DMA
    hbm = pl.BlockSpec(memory_space=pl.ANY)
    bf = jnp.bfloat16
    narrow = down.shape[1]
    group = nr * narrow
    downs = (part, plan.sp * narrow) if narrow % 128 == 0 else (plan.sp, part, narrow)
    proj = (2, plan.sp * tok, heads * NOPE)
    proj = pltpu.VMEM(proj if 4 * proj[1] * proj[2] < 2**23 + 1 else (8, 128), bf)
    more_c, more_x = max(nc - 1, 1), max(nx - 1, 1)
    more_r = max(nr - 1, 1)
    sizes = [(nz,), (nz, more_r), (nz, nr, more_x), (nz, nr, more_c), (3, nz), (3, nz, more_r)]
    sizes += [(more_c,), (more_x,), (5,), (nz, more_x), (nz, more_c)]
    sizes += [(nz, 2, more_c), (nz, 2, more_x), (nz, 3)]
    sems = [dma(size) for size in sizes for _ in range(2)]
    halves = 2 if nz > 1 else 1
    deep = nz // halves
    return pl.pallas_call(
        functools.partial(front_body, plan, heads, part),
        out_shape=jax.ShapeDtypeStruct((share, width), bf),
        in_specs=[hbm] * 17,
        out_specs=hbm,
        scratch_shapes=[
            pltpu.VMEM((share, width), jnp.float32),
            pltpu.VMEM((nz, nc, nx, share, width), bf),
            pltpu.VMEM((plan.sp * gate.shape[0], 2 * part), bf),
            pltpu.VMEM(downs, bf),
            pltpu.VMEM((plan.sp, nc, nx, share, kvl.shape[1] + 2 * ROPE), bf),
            pltpu.VMEM((tok, heads * VDIM), bf),
            *[pltpu.VMEM(small.shape, small.dtype) for small in args[:8]],
            pltpu.VMEM(wqp.shape, bf),
            pltpu.VMEM(wqr.shape, bf),
            pltpu.VMEM(wk.shape, bf),
            pltpu.VMEM(wv.shape, bf),
            pltpu.VMEM(wo.shape, bf),
            pltpu.VMEM((share, width), bf),
            pltpu.VMEM((heads, tok, NOPE + 2 * ROPE), bf),
            proj,
            pltpu.VMEM((nc, nx, share, width), bf),
            pltpu.VMEM((more_c, nx, share, width), bf),
            pltpu.VMEM((more_x, share, width), bf),
            pltpu.VMEM((more_x, share, width), bf),
            pltpu.VMEM((nz, tp * share, part), bf),
            pltpu.VMEM((nz, halves, nc, deep, nx, share, group), bf),
            pltpu.VMEM((nz, halves, more_c, deep, nx, share, group), bf),
            pltpu.VMEM((nz, halves, nx, deep, share, group), bf),
            pltpu.VMEM((nz, halves, more_x, deep, share, group), bf),
            *[pltpu.VMEM((nz, 3, share, group), bf)] * 2,
            pltpu.VMEM((share, width), bf),
            *sems,
            dma((19 + nz,)),
        ],
        compiler_params=pltpu.CompilerParams(
            collective_id=1, has_side_effects=True, vmem_limit_bytes=62 * 1024 * 1024
        ),
    )(*args)


def shards(
    plan,
    resid_in,
    query_latent,
    kv_latent,
    rotary_key,
    query_gain,
    kv_gain,
    w_query_plain,
    w_query_rotary,
    w_key_plain,
    w_value,
    w_output,
    ffn_gain,
    w_gate,
    w_up,
    w_down,
):
    tok = resid_in.shape[0]
    heads_dev = w_query_plain.shape[1] // NOPE
    hidden_dev = w_gate.shape[1]
    part = min(-(-hidden_dev // (plan.z * 128)) * 128, hidden_dev)

    offset = lax.axis_index("sp") * tok
    position = (offset + jnp.arange(tok, dtype=jnp.int32)).astype(jnp.float32)
    lane = lax.broadcasted_iota(jnp.int32, (1, 2 * ROPE), 1)
    index = lax.rem(lane, ROPE // 2) * 2
    freq = 10000.0 ** (-index.astype(jnp.float32) / ROPE)
    angle = position[:, None] * freq
    sign = jnp.where(lax.rem(lane, ROPE) < ROPE // 2, -1.0, 1.0)
    return front(
        plan,
        heads_dev,
        part,
        (
            query_latent,
            kv_latent,
            jnp.transpose(rotary_key),
            query_gain,
            kv_gain,
            jnp.cos(angle),
            jnp.sin(angle) * sign,
            ffn_gain,
            w_query_plain,
            w_query_rotary,
            w_key_plain,
            w_value,
            w_output,
            resid_in,
            w_gate,
            w_up,
            w_down,
        ),
    )


def solution(mesh):
    plan = Plan(mesh.shape["sp"], mesh.shape["tp"])
    return jax.shard_map(
        functools.partial(shards, plan),
        mesh=mesh,
        in_specs=(
            P("sp", None),
            P("sp", None),
            P("sp", None),
            P("sp", None),
            P(),
            P(),
            P(None, "tp"),
            P(None, "tp"),
            P(None, "tp"),
            P(None, "tp"),
            P("tp", None),
            P(),
            P("sp", "tp"),
            P("sp", "tp"),
            P("tp", "sp"),
        ),
        out_specs=P(("sp", "tp"), None),
        check_vma=False,
    )
```

```python
import functools

import jax
import jax.numpy as jnp
from jax import lax
from jax.experimental import pallas as pl
from jax.experimental.pallas import tpu as pltpu
from jax.sharding import PartitionSpec as P

NOPE = 128
ROPE = 64
VDIM = 128
MESH = pl.DeviceIdType.MESH


def normed(values, gain):
    wide = values.astype(jnp.float32)
    return wide * lax.rsqrt(jnp.mean(wide * wide, axis=-1, keepdims=True) + 1e-06) * gain


class Plan:
    def __init__(self, sp, tp):
        self.sp, self.tp = sp, tp
        self.z = 4 if sp % 4 == 0 else 1
        self.r = sp // self.z
        self.c = 2 if tp % 2 == 0 else 1
        self.x = tp // self.c

    def sizes(self):
        return {"z": self.z, "r": self.r, "x": self.x, "c": self.c}

    def here(self):
        s, t = lax.axis_index("sp"), lax.axis_index("tp")
        return {"z": s // self.r, "r": lax.rem(s, self.r), "x": t // self.c, "c": lax.rem(t, self.c)}

    def device(self, at):
        return {"sp": at["z"] * self.r + at["r"], "tp": at["x"] * self.c + at["c"]}

    def shifted(self, at, axis, by):
        size = self.sizes()[axis]
        return {**at, axis: lax.rem(at[axis] + (by % size), size)}

    def far(self):
        return (2, 3, 1) if self.z == 4 else ()

    def partner(self, at, m):
        z = at["z"]
        if m == 1:
            z = z + 1 - 2 * lax.rem(z, 2)
        elif m == 2:
            z = lax.rem(z + 2, 4)
        elif m == 3:
            z = 3 - z
        return {**at, "z": z}


def front_body(
    plan,
    heads,
    part,
    ql_hbm,
    kvl_hbm,
    rk_hbm,
    qg_hbm,
    kg_hbm,
    cos_hbm,
    sin_hbm,
    gain_hbm,
    wqp_hbm,
    wqr_hbm,
    wk_hbm,
    wv_hbm,
    wo_hbm,
    resid_hbm,
    gate_ref,
    up_ref,
    down_ref,
    o_ref,
    mid_ref,
    hn_ref,
    both_ref,
    downs_ref,
    packed,
    attn,
    ql_ref,
    kvl_ref,
    rk_ref,
    qg_ref,
    kg_ref,
    cos_ref,
    sin_ref,
    gain_ref,
    wqp_ref,
    wqr_ref,
    wk_ref,
    wv_ref,
    wo_ref,
    resid_ref,
    qcat,
    proj_ref,
    outp,
    swap_c,
    swap_s,
    swap_x,
    hidden,
    part_ref,
    got_c,
    sum_c,
    got_x,
    sum_z,
    got_z,
    done,
    kz_s,
    kz_r,
    ky_s,
    ky_r,
    kx_s,
    kx_r,
    kc_s,
    kc_r,
    wz_s,
    wz_r,
    wy_s,
    wy_r,
    sc_s,
    sc_r,
    sx_s,
    sx_r,
    hz_s,
    hz_r,
    hx_s,
    hx_r,
    hc_s,
    hc_r,
    fc_s,
    fc_r,
    fx_s,
    fx_r,
    fz_s,
    fz_r,
    local,
):
    here = plan.here()
    nz, nr, nx, nc, tp = plan.z, plan.r, plan.x, plan.c, plan.tp
    far = plan.far()
    z, r, x, c = here["z"], here["r"], here["x"], here["c"]
    latent = wk_ref.shape[0]
    depth, full = gate_ref.shape
    narrow = down_ref.shape[1]
    tok = ql_ref.shape[0]
    share = tok // tp
    sp_here, tp_here = lax.axis_index("sp"), lax.axis_index("tp")
    wide, bf = jnp.float32, jnp.bfloat16
    f32 = wide
    waits = []

    def drain():
        while waits:
            waits.pop().wait_send()

    def peer(axis, by):
        return plan.device(plan.shifted(here, axis, by))

    def zpeer(m):
        return plan.device(plan.partner(here, m))

    def zof(m):
        return plan.partner(here, m)["z"]

    barrier = pltpu.get_barrier_semaphore()
    peers = [zpeer(m) for m in far]
    for axis, size in (("r", nr), ("x", nx), ("c", nc)):
        peers += [peer(axis, k) for k in range(1, size)]
    for to in peers:
        pl.semaphore_signal(barrier, inc=1, device_id=to, device_id_type=MESH)

    smalls = [
        (kvl_hbm, kvl_ref),
        (kg_hbm, kg_ref),
        (rk_hbm, rk_ref),
        (cos_hbm, cos_ref),
        (sin_hbm, sin_ref),
        (ql_hbm, ql_ref),
        (qg_hbm, qg_ref),
        (gain_hbm, gain_ref),
    ]
    base = 11 + nz
    smalls = [pltpu.make_async_copy(s, d, local.at[base + i]) for i, (s, d) in enumerate(smalls)]
    for copy in smalls:
        copy.start()
    loads = [
        (wqp_hbm, wqp_ref),
        (wqr_hbm, wqr_ref),
        (wk_hbm, wk_ref),
        (wv_hbm, wv_ref),
        (wo_hbm, wo_ref),
        (resid_hbm.at[pl.ds(pl.multiple_of(tp_here * share, share), share)], resid_ref),
    ]
    loads = [pltpu.make_async_copy(s, d, local.at[i]) for i, (s, d) in enumerate(loads)]
    for copy in loads:
        copy.start()

    def send(src, dst, device, sem_s, sem_r):
        copy = pltpu.make_async_remote_copy(
            src_ref=src,
            dst_ref=dst,
            send_sem=sem_s,
            recv_sem=sem_r,
            device_id=device,
            device_id_type=MESH,
        )
        copy.start()
        waits.append(copy)
        return copy

    pair = 2 * ROPE
    lane = lax.broadcasted_iota(jnp.int32, (1, pair), 1)
    first = lax.rem(lane, ROPE) < ROPE // 2

    def rotated(v):
        other = jnp.where(first, pltpu.roll(v, pair - ROPE // 2, 1), pltpu.roll(v, ROPE // 2, 1))
        return (v * cos_ref[...] + other * sin_ref[...]).astype(bf)

    def block_of(at):
        return at["z"] * nr + at["r"]

    for copy in smalls[:5]:
        copy.wait()
    with jax.named_scope("kvprep"):
        lat = normed(kvl_ref[...], kg_ref[...][None, :]).astype(bf)
        raw = rk_ref[...].astype(f32)
        rot = rotated(jnp.concatenate([raw, raw], axis=0).T)
        for i in range(tp):
            rows = slice(i * share, (i + 1) * share)
            packed[sp_here, i % nc, i // nc, :, :latent] = lat[rows]
            packed[sp_here, i % nc, i // nc, :, latent:] = rot[rows]

    with jax.named_scope("barrier"):
        pl.semaphore_wait(barrier, len(peers))

    kz, ky, kx, kc = {}, {}, {}, {}

    def kv_at(m, j):
        return block_of(plan.shifted(plan.partner(here, m), "r", -j))

    def kv_y(m):
        q = packed.at[kv_at(m, 0), c]
        q = q if m == 0 else q.at[x]
        for j in range(1, nr):
            ky[m, j] = send(q, q, peer("r", j), ky_s.at[m, j - 1], ky_r.at[m, j - 1])

    def kv_x(m, j):
        for l in range(1, nx):
            q = packed.at[kv_at(m, j), c, x]
            kx[m, j, l] = send(q, q, peer("x", l), kx_s.at[m, j, l - 1], kx_r.at[m, j, l - 1])

    def kv_c(m, j):
        for l in range(1, nx):
            if (m, j, l) in kx:
                kx[m, j, l].wait_recv()
        for l in range(1, nc):
            q = packed.at[kv_at(m, j), c]
            kc[m, j, l] = send(q, q, peer("c", l), kc_s.at[m, j, l - 1], kc_r.at[m, j, l - 1])

    own = packed.at[sp_here, c]
    for m in far:
        q = own if m == 1 else own.at[x]
        kz[m] = send(q, q, zpeer(m), kz_s.at[m], kz_r.at[m])
    kv_y(0)

    def window(index):
        return pl.multiple_of(jnp.minimum(index * part, full - part), 128)

    def targets(sp):
        rows = pl.ds(pl.multiple_of(sp * depth, depth), depth)
        if len(downs_ref.shape) == 3:
            downs = downs_ref.at[sp]
        else:
            downs = downs_ref.at[:, pl.ds(pl.multiple_of(sp * narrow, 128), narrow)]
        return [
            both_ref.at[rows, pl.ds(0, part)],
            both_ref.at[rows, pl.ds(part, part)],
            downs,
        ]

    def sources(index):
        lanes = pl.ds(window(index), part)
        return [gate_ref.at[:, lanes], up_ref.at[:, lanes], down_ref.at[lanes, :]]

    over_z, over_r = {}, {}
    streams = []
    mine = []

    for w in range(3):
        for m in far:
            over_z[w, m] = pltpu.make_async_remote_copy(
                src_ref=sources(zof(m))[w],
                dst_ref=targets(sp_here)[w],
                send_sem=wz_s.at[w, m],
                recv_sem=wz_r.at[w, m],
                device_id=zpeer(m),
                device_id_type=MESH,
            )

    inside = lax.rem(z, 3) != 0
    outside = lax.rem(z, 3) == 0

    def spread(w, *ms):
        for m in ms:
            if m in far:
                over_z[w, m].start()

    def spread_if(when, w, *ms):
        @pl.when(when)
        def _():
            spread(w, *ms)

    def arrange(w, m):
        dst = targets(kv_at(m, 0))[w]
        src = dst if m else sources(z)[w]
        for j in range(1, nr):
            over_r[w, m, j] = pltpu.make_async_remote_copy(
                src_ref=src,
                dst_ref=dst,
                send_sem=wy_s.at[w, m, j - 1],
                recv_sem=wy_r.at[w, m, j - 1],
                device_id=peer("r", j),
                device_id_type=MESH,
            )
            streams.append(over_r[w, m, j])

    def go(w, m):
        if m:
            over_z[w, m].wait_recv()
        for j in range(1, nr):
            over_r[w, m, j].start()

    def forward(w, m):
        arrange(w, m)
        go(w, m)

    for w in range(3):
        for m in far:
            over_z[w, m] = pltpu.make_async_remote_copy(
                src_ref=sources(zof(m))[w],
                dst_ref=targets(sp_here)[w],
                send_sem=wz_s.at[w, m],
                recv_sem=wz_r.at[w, m],
                device_id=zpeer(m),
                device_id_type=MESH,
            )

    inside = lax.rem(z, 3) != 0
    outside = lax.rem(z, 3) == 0

    def spread(w, *ms):
        for m in ms:
            if m in far:
                over_z[w, m].start()

    def spread_if(when, w, *ms):
        @pl.when(when)
        def _():
            spread(w, *ms)

    def forward(w, m):
        dst = targets(kv_at(m, 0))[w]
        src = dst if m else sources(z)[w]
        if m:
            over_z[w, m].wait_recv()
        for j in range(1, nr):
            over_r[w, m, j] = send(src, dst, peer("r", j), wy_s.at[w, m, j - 1], wy_r.at[w, m, j - 1])
            streams.append(waits.pop())

    for w in range(3):
        mine.append(pltpu.make_async_copy(sources(z)[w], targets(sp_here)[w], local.at[8 + w]))
        mine[-1].start()

    early = len(proj_ref.shape) == 3

    def project(sp):
        if early:
            kv = packed[sp, :, :, :, :latent].reshape(tok, latent)
            for i, w_ref in enumerate((wk_ref, wv_ref)):
                out = jnp.dot(kv, w_ref[...], preferred_element_type=f32)
                proj_ref[i, pl.ds(pl.multiple_of(sp * tok, tok), tok), :] = out.astype(bf)

    with jax.named_scope("qprep"):
        for copy in smalls[5:]:
            copy.wait()
        qn = normed(ql_ref[...], qg_ref[...][None, :]).astype(bf)
        loads[0].wait()
        loads[1].wait()
        plain = jnp.dot(qn, wqp_ref[...], preferred_element_type=f32).astype(bf)
        turned = jnp.dot(qn, wqr_ref[...], preferred_element_type=f32)
        for h in range(heads):
            p = h // 2 * pair
            both = rotated(turned[:, p : p + pair])
            keep = (lane >= ROPE) if h % 2 else (lane < ROPE)
            qcat[h, :, :NOPE] = plain[:, h * NOPE : (h + 1) * NOPE]
            qcat[h, :, NOPE:] = jnp.where(keep, both.astype(f32), 0.0).astype(bf)

    loads[2].wait()
    loads[3].wait()
    with jax.named_scope("projown"):
        project(sp_here)
    with jax.named_scope("kvz"):
        for m in far:
            kz[m].wait_recv()
            kv_y(m)
            if m == 1:
                kv_c(m, 0)
            else:
                kv_x(m, 0)
    spread(0, *far)
    spread_if(inside, 1, 2, 1)
    spread_if(outside, 1, 3, 1)
    near = [(0, j) for j in range(1, nr)] + [(1, 0)][: len(far)]
    rest = [(m, 0) for m in far if m != 1]
    late = [(m, j) for j in range(1, nr) for m in far]

    def landed(keys):
        for m, j in keys:
            for l in range(1, nc):
                kc[m, j, l].wait_recv()
            project(kv_at(m, j))

    with jax.named_scope("kvy"):
        for j in range(1, nr):
            ky[0, j].wait_recv()
            kv_c(0, j)
        for m, j in late:
            ky[m, j].wait_recv()
            kv_x(m, j)
    with jax.named_scope("near"):
        landed(near)
    with jax.named_scope("kvc"):
        for m, j in rest:
            kv_c(m, j)
        with jax.named_scope("kvcl"):
            landed(rest)
    with jax.named_scope("kvlate"):
        for key in late:
            kv_c(*key)
        for w in range(2):
            forward(w, 0)
        landed(late)

    scale = (NOPE + ROPE) ** (-0.5)
    count = plan.sp * tok

    def transposed(left, right):
        return lax.dot_general(
            left, right, (((1,), (1,)), ((), ())), preferred_element_type=f32
        )

    def head(h):
        lanes = pl.ds(pl.multiple_of(h * NOPE, NOPE), NOPE)
        rot = packed[:, :, :, :, latent:].reshape(count, pair)
        if early:
            plain, vals = proj_ref[0, :, lanes], proj_ref[1, :, lanes]
        else:
            kv = packed[:, :, :, :, :latent].reshape(count, latent)
            weights = jnp.concatenate([wk_ref[:, lanes], wv_ref[:, lanes]], axis=1)
            mixed = jnp.dot(kv, weights, preferred_element_type=f32).astype(bf)
            plain, vals = mixed[:, :NOPE], mixed[:, NOPE:]
        score = transposed(qcat[h], jnp.concatenate([plain, rot], axis=1)) * scale
        weight = jnp.exp(score - jnp.max(score, axis=-1, keepdims=True))
        total = jnp.sum(weight, axis=-1, keepdims=True)
        value = jnp.dot(weight.astype(bf), vals, preferred_element_type=f32)
        attn[:, lanes] = (value / total).astype(bf)

    todo = [(0, m) for m in far]

    def pump(n):
        for _ in range(n):
            if todo:
                forward(*todo.pop(0))

    @pl.loop(0, heads)
    def _(h):
        with jax.named_scope("head"):
            head(h)

    with jax.named_scope("pump0"):
        pump(PUMPS[0])
    with jax.named_scope("outproj"):
        loads[4].wait()
        loads[5].wait()
        term = jnp.dot(attn[...], wo_ref[...], preferred_element_type=f32).astype(bf)
        for i in range(tp):
            outp[i % nc, i // nc] = term[i * share : (i + 1) * share]
    swaps_c = [
        send(
            outp.at[lax.rem(c + l, nc)], swap_c.at[l - 1], peer("c", l), sc_s.at[l - 1], sc_r.at[l - 1]
        )
        for l in range(1, nc)
    ]
    with jax.named_scope("swapc"):
        for copy in swaps_c:
            copy.wait_recv()

    def folded(i):
        total = outp[c, i].astype(f32)
        for l in range(1, nc):
            total += swap_c[l - 1, i].astype(f32)
        return total

    swaps_x = []
    for l in range(1, nx):
        i = lax.rem(x + l, nx)
        swap_s[l - 1] = folded(i).astype(bf)
        swaps_x.append(
            send(swap_s.at[l - 1], swap_x.at[l - 1], peer("x", l), sx_s.at[l - 1], sx_r.at[l - 1])
        )
    mid = resid_ref[...].astype(f32) + folded(x)
    with jax.named_scope("pumpA"):
        pump(PUMPS[1])
    drain()
    with jax.named_scope("swapx"):
        for l, copy in enumerate(swaps_x):
            copy.wait_recv()
            mid += swap_x[l].astype(f32)
    mid_ref[...] = mid
    hn_ref[z, c, x] = (
        mid * lax.rsqrt(jnp.mean(mid * mid, axis=-1, keepdims=True) + 1e-06) * gain_ref[...][None, :]
    ).astype(bf)

    hz, hx, hc = {}, {}, {}
    order = (0,) + tuple(range(1, nz))
    half = z // 2
    origin = (z, z + 1 - 2 * lax.rem(z, 2), 2 - half, 3 - 3 * half)[:nz]
    inner_z = inside

    def hn_z(k, device, at):
        q = hn_ref.at[origin[k], c, x]
        return pltpu.make_async_remote_copy(
            src_ref=q,
            dst_ref=q,
            send_sem=hz_s.at[{(0, 1): 0, (0, 2): 1, (1, 3): 2, (2, 2): 3, (3, 3): 4}.get((k, at), 0)],
            recv_sem=hz_r.at[at],
            device_id=device,
            device_id_type=MESH,
        )

    def hn_send(copy, when=None):
        @pl.when(inner_z if when is None else when)
        def _():
            copy.start()

        hops.append(copy)

    hops = []

    def hn_x(k):
        q = hn_ref.at[origin[k], c, x]
        for l in range(1, nx):
            hx[k, l] = send(q, q, peer("x", l), hx_s.at[k, l - 1], hx_r.at[k, l - 1])

    for k in order:
        q = hn_ref.at[origin[k], c]
        for l in range(1, nc):
            hc[k, l] = pltpu.make_async_remote_copy(
                src_ref=q,
                dst_ref=q,
                send_sem=hc_s.at[k, l - 1],
                recv_sem=hc_r.at[k, l - 1],
                device_id=peer("c", l),
                device_id_type=MESH,
            )
            waits.append(hc[k, l])

    def hn_c(k):
        for l in range(1, nx):
            hx[k, l].wait_recv()
        for l in range(1, nc):
            hc[k, l].start()

    place = z * part
    lanes = lax.broadcasted_iota(jnp.int32, (1, part), 1)
    fresh = lanes >= place - jnp.minimum(place, full - part)

    def inner(k):
        for l in range(1, nc):
            hc[k, l].wait_recv()
        rows = hn_ref[origin[k]].reshape(tp * share, -1)
        both = jnp.dot(rows, both_ref[...], preferred_element_type=f32)
        value = jnp.where(fresh, jax.nn.silu(both[:, :part]) * both[:, part:], 0.0)
        hidden[origin[k]] = value.astype(bf)

    def ready():
        for w in range(2):
            mine[w].wait()
            for m in (0,) + far:
                for j in range(1, nr):
                    over_r[w, m, j].wait_recv()

    inside_i = jnp.minimum(lax.rem(z, 3), 1)
    groups = origin
    sender = (0,) + ((1, 2 + inside_i, 3 - inside_i) if nz > 1 else ())
    down_r = {}

    def remote(src, dst, device, sem_s, sem_r):
        return pltpu.make_async_remote_copy(
            src_ref=src,
            dst_ref=dst,
            send_sem=sem_s,
            recv_sem=sem_r,
            device_id=device,
            device_id_type=MESH,
        )

    def down(i):
        dst = targets(groups[i] * nr + r)[2]
        m = sender[i]
        remote(dst, dst, zpeer(1), wz_s.at[2, m], wz_r.at[2, m]).wait_recv()
        for j in range(1, nr):
            down_r[i, j] = send(dst, dst, peer("r", j), wy_s.at[2, m, j - 1], wy_r.at[2, m, j - 1])

    for m in far:
        arrange(1, m)

    def ups(when, *ms):
        @pl.when(when)
        def _():
            for m in ms:
                go(1, m)

    if nz > 1:
        direct = hn_z(0, zpeer(1), 1)
        direct.start()
        waits.append(direct)
        hn_send(hn_z(0, zpeer(3), 2))
        spread_if(inside, 1, 3)
    hn_x(0)
    if nz > 1:
        with jax.named_scope("upsout"):
            ups(outside, 2, 1, 3)
            ups(inside, 1)
    forward(2, 0)
    if nz > 1:
        with jax.named_scope("hn1"):
            hn_z(1, zpeer(1), 1).wait_recv()
            hn_send(hn_z(1, zpeer(3), 3))
            hn_x(1)
        spread_if(outside, 1, 2)
        spread_if(outside, 2, 1)
        with jax.named_scope("hnc0"):
            hn_c(0)
        with jax.named_scope("hn2"):
            hn_z(2, zpeer(1), 2).wait_recv()
            hn_send(hn_z(2, zpeer(1), 2))
            hn_x(2)
        with jax.named_scope("upsin2"):
            ups(inside, 3, 2)
        with jax.named_scope("hnc1"):
            hn_c(1)
        spread_if(inside, 2, 1)
        with jax.named_scope("down1"):
            down(1)
        with jax.named_scope("hn3"):
            hn_z(3, zpeer(1), 3).wait_recv()
            hn_send(hn_z(3, zpeer(1), 3))
            hn_x(3)
        spread_if(outside, 2, 2, 3)
        spread_if(inside, 2, 3)
    else:
        hn_c(0)

    group = nr * narrow
    halves = 2 if nz > 1 else 1
    deep = nz // halves
    bases = (2 * half, 2 - 2 * half)[:halves] if nz > 1 else (0,)
    landing = {1: ((1, 0, 2, 3),) * 2, 2: ((3, 2, 0, 1), (2, 3, 1, 0)), 3: ((3, 2, 1, 0), (2, 3, 0, 1))}
    away = []
    over_c, over_x, back = {}, {}, {}

    def columns_of(i):
        return pl.ds(pl.multiple_of(groups[i] * group, 128), group)

    fed = set()

    def feed(i, f):
        if i not in fed:
            fed.add(i)
            if i == 0:
                mine[2].wait()
            for j in range(1, nr):
                (down_r[i, j] if i else over_r[2, 0, j]).wait_recv()
        rows = hidden[pl.ds(bases[f], deep)].reshape(deep * tp * share, part)

        def keep(piece, columns):
            piece = piece.astype(bf).reshape(deep, nc, nx, share, -1)
            for k in range(nc):
                part_ref[i, f, k, :, :, :, columns] = piece[:, k]

        if len(downs_ref.shape) == 3:
            for k in range(nr):
                piece = jnp.dot(rows, downs_ref[groups[i] * nr + k], preferred_element_type=f32)
                keep(piece, slice(k * narrow, (k + 1) * narrow))
        else:
            keep(jnp.dot(rows, downs_ref[:, columns_of(i)], preferred_element_type=f32), slice(None))
        for l in range(1, nc):
            over_c[i, f, l] = send(
                part_ref.at[i, f, lax.rem(c + l, nc)],
                got_c.at[i, f, l - 1],
                peer("c", l),
                fc_s.at[i, f, l - 1],
                fc_r.at[i, f, l - 1],
            )

    def fold_c(i, f):
        for l in range(1, nc):
            over_c[i, f, l].wait_recv()
        for k in range(1, nx + 1):
            to = lax.rem(x + k, nx)
            total = part_ref[i, f, c, :, to].astype(f32)
            for l in range(1, nc):
                total += got_c[i, f, l - 1, :, to].astype(f32)
            sum_c[i, f, to] = total.astype(bf)
            if k < nx:
                over_x[i, f, k] = send(
                    sum_c.at[i, f, to],
                    got_x.at[i, f, k - 1],
                    peer("x", k),
                    fx_s.at[i, f, k - 1],
                    fx_r.at[i, f, k - 1],
                )

    def fold_x(i, f):
        for k in range(1, nx):
            over_x[i, f, k].wait_recv()

        def total(q):
            value = sum_c[i, f, x, q].astype(f32)
            for k in range(1, nx):
                value += got_x[i, f, k - 1, q].astype(f32)
            return value

        def ship(m, q):
            at, to = (table[i] for table in landing[m])
            k = at + inside_i * (to - at)
            sum_z[i, m - 1] = total(q).astype(bf)
            back[i, m] = send(
                sum_z.at[i, m - 1],
                got_z.at[k, m - 1],
                zpeer(m),
                fz_s.at[i, m - 1],
                fz_r.at[k, m - 1],
            )

        if f == 0:
            if nz > 1:
                ship(1, 1 - lax.rem(z, 2))
            mid_ref[:, columns_of(i)] += total(lax.rem(z, deep))
        else:
            for m in (2, 3):
                ship(m, plan.partner(here, m)["z"] - bases[1])

    def close(i):
        total = mid_ref[:, columns_of(i)]
        if nz > 1:
            for m in far:
                q = got_z.at[i, m - 1]
                remote(q, q, zpeer(m), fz_s.at[i, m - 1], fz_r.at[i, m - 1]).wait_recv()
                total += got_z[i, m - 1].astype(f32)
        done[:, columns_of(i)] = total.astype(bf)
        away.append(pltpu.make_async_copy(done.at[:, columns_of(i)], o_ref.at[:, columns_of(i)], local.at[11 + i]))
        away[-1].start()

    def settle(i):
        for copy in over_z.values():
            copy.wait_send()
        for copy in hops:

            @pl.when(inner_z)
            def _():
                copy.wait_send()

        for copy in streams:
            copy.wait_send()
        early_ids = {id(copy) for copy in settled}
        waits[:] = [copy for copy in waits if id(copy) not in early_ids]
        for copy in settled:
            copy.wait_send()

    def step(stage, *key):
        if key[0] < nz and (len(key) < 2 or key[1] < halves):
            with jax.named_scope(stage.__name__ + "_".join(map(str, key))):
                stage(*key)

    def last(when):
        if nz > 1:

            @pl.when(when)
            def _():
                with jax.named_scope("hnc3"):
                    hn_c(3)

    if nz > 1:
        with jax.named_scope("hnc2"):
            hn_c(2)
    last(inside)
    with jax.named_scope("gateup"):
        ready()
    spread_if(inside, 2, 2)
    step(inner, 0)
    step(inner, 1)
    step(feed, 0, 0)
    step(inner, 2)
    step(fold_c, 0, 0)
    step(feed, 1, 0)
    last(outside)
    step(fold_c, 1, 0)
    step(inner, 3)
    step(feed, 0, 1)
    step(feed, 1, 1)
    step(fold_c, 0, 1)
    step(fold_c, 1, 1)
    step(fold_x, 0, 0)
    step(down, 2)
    step(fold_x, 1, 0)
    step(fold_x, 0, 1)
    settled = list(waits)
    step(down, 3)
    step(fold_x, 1, 1)
    step(feed, 2, 1)
    step(feed, 2, 0)
    step(fold_c, 2, 1)
    step(fold_c, 2, 0)
    step(feed, 3, 1)
    step(feed, 3, 0)
    step(fold_c, 3, 1)
    step(fold_c, 3, 0)
    step(settle, 0)
    step(fold_x, 2, 1)
    step(fold_x, 2, 0)
    step(fold_x, 3, 1)
    step(fold_x, 3, 0)
    for i in range(4):
        step(close, i)
    drain()
    for copy in away:
        copy.wait()


PUMPS = (1, 2)


def front(plan, heads, part, args):
    nz, nr, nx, nc, tp = plan.z, plan.r, plan.x, plan.c, plan.tp
    ql, kvl = args[0], args[1]
    wqp, wqr, wk, wv, wo, resid, gate, up, down = args[8:]
    tok, width = resid.shape
    share = tok // tp
    dma = pltpu.SemaphoreType.DMA
    hbm = pl.BlockSpec(memory_space=pl.ANY)
    bf = jnp.bfloat16
    narrow = down.shape[1]
    group = nr * narrow
    downs = (part, plan.sp * narrow) if narrow % 128 == 0 else (plan.sp, part, narrow)
    proj = (2, plan.sp * tok, heads * NOPE)
    proj = pltpu.VMEM(proj if 4 * proj[1] * proj[2] < 2**23 + 1 else (8, 128), bf)
    more_c, more_x = max(nc - 1, 1), max(nx - 1, 1)
    more_r = max(nr - 1, 1)
    sizes = [(nz,), (nz, more_r), (nz, nr, more_x), (nz, nr, more_c), (3, nz), (3, nz, more_r)]
    sizes += [(more_c,), (more_x,), (5,), (nz, more_x), (nz, more_c)]
    sizes += [(nz, 2, more_c), (nz, 2, more_x), (nz, 3)]
    sems = [dma(size) for size in sizes for _ in range(2)]
    halves = 2 if nz > 1 else 1
    deep = nz // halves
    return pl.pallas_call(
        functools.partial(front_body, plan, heads, part),
        out_shape=jax.ShapeDtypeStruct((share, width), bf),
        in_specs=[hbm] * 17,
        out_specs=hbm,
        scratch_shapes=[
            pltpu.VMEM((share, width), jnp.float32),
            pltpu.VMEM((nz, nc, nx, share, width), bf),
            pltpu.VMEM((plan.sp * gate.shape[0], 2 * part), bf),
            pltpu.VMEM(downs, bf),
            pltpu.VMEM((plan.sp, nc, nx, share, kvl.shape[1] + 2 * ROPE), bf),
            pltpu.VMEM((tok, heads * VDIM), bf),
            *[pltpu.VMEM(small.shape, small.dtype) for small in args[:8]],
            pltpu.VMEM(wqp.shape, bf),
            pltpu.VMEM(wqr.shape, bf),
            pltpu.VMEM(wk.shape, bf),
            pltpu.VMEM(wv.shape, bf),
            pltpu.VMEM(wo.shape, bf),
            pltpu.VMEM((share, width), bf),
            pltpu.VMEM((heads, tok, NOPE + 2 * ROPE), bf),
            proj,
            pltpu.VMEM((nc, nx, share, width), bf),
            pltpu.VMEM((more_c, nx, share, width), bf),
            pltpu.VMEM((more_x, share, width), bf),
            pltpu.VMEM((more_x, share, width), bf),
            pltpu.VMEM((nz, tp * share, part), bf),
            pltpu.VMEM((nz, halves, nc, deep, nx, share, group), bf),
            pltpu.VMEM((nz, halves, more_c, deep, nx, share, group), bf),
            pltpu.VMEM((nz, halves, nx, deep, share, group), bf),
            pltpu.VMEM((nz, halves, more_x, deep, share, group), bf),
            *[pltpu.VMEM((nz, 3, share, group), bf)] * 2,
            pltpu.VMEM((share, width), bf),
            *sems,
            dma((19 + nz,)),
        ],
        compiler_params=pltpu.CompilerParams(
            collective_id=1, has_side_effects=True, vmem_limit_bytes=62 * 1024 * 1024
        ),
    )(*args)


def shards(
    plan,
    resid_in,
    query_latent,
    kv_latent,
    rotary_key,
    query_gain,
    kv_gain,
    w_query_plain,
    w_query_rotary,
    w_key_plain,
    w_value,
    w_output,
    ffn_gain,
    w_gate,
    w_up,
    w_down,
):
    tok = resid_in.shape[0]
    heads_dev = w_query_plain.shape[1] // NOPE
    hidden_dev = w_gate.shape[1]
    part = min(-(-hidden_dev // (plan.z * 128)) * 128, hidden_dev)

    offset = lax.axis_index("sp") * tok
    position = (offset + jnp.arange(tok, dtype=jnp.int32)).astype(jnp.float32)
    lane = lax.broadcasted_iota(jnp.int32, (1, 2 * ROPE), 1)
    index = lax.rem(lane, ROPE // 2) * 2
    freq = 10000.0 ** (-index.astype(jnp.float32) / ROPE)
    angle = position[:, None] * freq
    sign = jnp.where(lax.rem(lane, ROPE) < ROPE // 2, -1.0, 1.0)
    return front(
        plan,
        heads_dev,
        part,
        (
            query_latent,
            kv_latent,
            jnp.transpose(rotary_key),
            query_gain,
            kv_gain,
            jnp.cos(angle),
            jnp.sin(angle) * sign,
            ffn_gain,
            w_query_plain,
            w_query_rotary,
            w_key_plain,
            w_value,
            w_output,
            resid_in,
            w_gate,
            w_up,
            w_down,
        ),
    )


def solution(mesh):
    plan = Plan(mesh.shape["sp"], mesh.shape["tp"])
    return jax.shard_map(
        functools.partial(shards, plan),
        mesh=mesh,
        in_specs=(
            P("sp", None),
            P("sp", None),
            P("sp", None),
            P("sp", None),
            P(),
            P(),
            P(None, "tp"),
            P(None, "tp"),
            P(None, "tp"),
            P(None, "tp"),
            P("tp", None),
            P(),
            P("sp", "tp"),
            P("sp", "tp"),
            P("tp", "sp"),
        ),
        out_specs=P(("sp", "tp"), None),
        check_vma=False,
    )
```
